32 devices in a mesh: ep: 4 (over y, x), tp: 8 (over z, core).
Axes of the slice: x: 2, y: 2, z: 4, core: 2. Of those that a mesh axis runs over, the one named last changes fastest.
Arguments:
- mixer_input_rows: bfloat16 [4096, 2048], P(('ep', 'tp')), may hold values from -6 to 6
- mixer_norm_gain: float32 [2048], replicated, may hold values from 0.1 to 1.9
- query_weight: bfloat16 [2048, 2048], P(None, 'tp'), may hold values from -0.125 to 0.125
- key_weight: bfloat16 [2048, 2048], P(None, 'tp'), may hold values from -0.125 to 0.125
- value_weight: bfloat16 [2048, 2048], P(None, 'tp'), may hold values from -0.125 to 0.125
- write_strength_projection: bfloat16 [2048, 16], replicated, may hold values from -0.125 to 0.125
- decay_projection: bfloat16 [2048, 16], replicated, may hold values from -0.125 to 0.125
- head_decay_speed: float32 [16], P('tp'), may hold values from 0 to 1
- largest_write_strength: float32 [16], P('tp'), may hold values from 0 to 1
- extra_log_decay: float32 [4096, 16], P('ep', 'tp'), may hold values from -1 to 0
- head_norm_gain: float32 [128], replicated, may hold values from 0.1 to 1.9
- mixer_output_weight: bfloat16 [2048, 2048], P('tp'), may hold values from -0.125 to 0.125
- expert_input_rows: bfloat16 [256, 2048], P(('ep', 'tp')), may hold values from -6 to 6
- expert_norm_gain: float32 [2048], replicated, may hold values from 0.1 to 1.9
- routes: int32 [256, 2], P(('ep', 'tp')), may hold values from 0 to 3, all different within a row; in each aligned block of 8 rows (0 to 7, 8 to 15, ...) at most 6 rows name the same one
- expert_route_weight: float32 [256, 2], P(('ep', 'tp')), may hold values from 0.2 to 1
- gate_weight: bfloat16 [4, 2048, 7168], P('ep', None, 'tp'), may hold values from -0.125 to 0.125
- up_weight: bfloat16 [4, 2048, 7168], P('ep', None, 'tp'), may hold values from -0.125 to 0.125
- down_weight: bfloat16 [4, 7168, 2048], P('ep', 'tp'), may hold values from -0.0625 to 0.0625
Outputs:
- mix_out: bfloat16 [4096, 2048], P(('ep', 'tp'))
- exp_out: bfloat16 [256, 2048], P(('ep', 'tp'))
The draws below stay inside these ranges and needn't reach their ends.
Inputs may be any that keep to these rules, and one draw needn't show every extreme that they name: `routes`: within the rows of one device (aligned blocks of 8 rows) no expert is named more than 6 times, some device names some expert exactly 6 times, and the 2 experts of a row differ.
All inputs are finite; a program needn't handle non-finite values.
Results may differ from the reference program's by a relative error of at most 0.019.
Values may be sent and summed in bfloat16 or wider, within the bound.
A program may use at most 128 MiB of HBM per device.

```python
import math
import jax
import jax.numpy as jnp
import numpy as np
from jax import lax

D = 2048
HEADS = 16
HEAD = 128
FF = 7168
BLOCK = 128
TOP = 2
EXP_TOK_DEV = 8
HEADS_DEV = 2
FF_DEV = 896
SPAN_EP = 1024
SEQ = 4096
EXP_TOKENS = 256
EXPERTS = 4
CAP = 6
N_EP = 4
N_TP = 8


def head_split(key):
    ranks = jax.random.permutation(jax.random.fold_in(key, 101), HEADS)
    quick_count = HEADS // 2
    return ranks < quick_count


def draw_head_decay_speed(key, part):
    quick = head_split(key)
    fast_rate = jax.random.uniform(jax.random.fold_in(key, 102), (HEADS,), jnp.float32, 0.025, 0.05)
    slow_rate = jax.random.uniform(jax.random.fold_in(key, 103), (HEADS,), jnp.float32, 0.1, 0.3) / SEQ
    return jnp.where(quick, fast_rate, slow_rate)


def draw_largest_write_strength(key, part):
    quick = head_split(key)
    fast_rate = jax.random.uniform(jax.random.fold_in(key, 104), (HEADS,), jnp.float32, 0.6, 1.0)
    slow_rate = jax.random.uniform(jax.random.fold_in(key, 105), (HEADS,), jnp.float32, 0.5, 1.0) * HEAD / SEQ
    return jnp.where(quick, fast_rate, slow_rate)


def draw_extra_log_decay(key, part):
    span_count = SEQ // SPAN_EP
    position = jnp.arange(SEQ)
    steady = jax.random.uniform(jax.random.fold_in(key, 111), (span_count, HEADS), jnp.float32, 0.12, 0.5)
    level = -steady[position // SPAN_EP] / SEQ
    spots = jax.random.randint(jax.random.fold_in(key, 112), (3,), 0, SEQ)
    drops = jnp.log(jax.random.uniform(jax.random.fold_in(key, 113), (3, HEADS), jnp.float32, 0.6, 0.8))
    hits = (position[:, None] == spots[None, :]).astype(jnp.float32)
    return level + jnp.sum(hits[:, :, None] * drops[None, :, :], axis=1)


def shard_levels(own_key, extent, shards, smallest, top_value):
    factor_of, own = 1.0, jax.random.fold_in(own_key, 6)
    for dim, shards_of in shards:
        steps = jnp.exp(jax.random.uniform(jax.random.fold_in(own, dim), (shards_of,), jnp.float32, smallest / len(shards), top_value / len(shards)))
        factor_of = factor_of * jnp.repeat(steps, extent[dim] // shards_of).reshape([-1 if axis == dim else 1 for axis in range(len(extent))])
    return factor_of


def routed_block(stream_key, own, number, rows, count, top, limit, slope):
    order = jax.random.permutation(stream_key, count)
    packed, common = load_shares(count, rows * top, limit, slope, True), load_shares(count, rows * top, limit, slope, False)
    places = jnp.arange(count)

    def named(tallies, offset_by):
        used = int((tallies > 0).sum())
        fixed = max(1, used // 4)
        passed = fixed + (places - fixed + offset_by * (used - fixed)) % max(1, count - fixed)
        return jnp.zeros((count,), jnp.int32).at[order[jnp.where(places < fixed, places, passed)]].set(jnp.asarray(tallies, jnp.int32))

    tallies = jnp.where(number % 4 == 0, named(packed, number // 4), named(common, number - number // 4 - 1))
    mixed = jax.random.permutation(jax.random.fold_in(own, 3), count)
    source_of, taker = mixed[0:count // 2 * 2:2], mixed[1:count // 2 * 2:2]
    margin = jnp.minimum(tallies[source_of] - 1, limit - tallies[taker]) // 2
    margin = jnp.where((source_of == order[0]) | (taker == order[0]) | (tallies[taker] == 0), 0, jnp.maximum(margin, 0))
    passed = jax.random.randint(jax.random.fold_in(own, 4), (count // 2,), 0, 1 << 20) % (margin + 1)
    tallies = tallies.at[source_of].add(-passed).at[taker].add(passed)
    members = jnp.searchsorted(jnp.cumsum(tallies), jnp.arange(rows * top), side="right").astype(jnp.int32)
    listing = members.reshape(top, rows).T
    listing = listing[jax.random.permutation(jax.random.fold_in(own, 1), rows)]
    offset_by = jax.random.randint(jax.random.fold_in(own, 2), (rows, 1), 0, top)
    return jnp.take_along_axis(listing, (jnp.arange(top)[None, :] + offset_by) % top, axis=1)


def load_shares(number_of, total, reach, lean, full):
    portions = [(1 << 20) // math.isqrt(rank ** lean) + 1 for rank in range(1, number_of + 1)]
    largest = reach if full else min(reach, max(-(-total // number_of), total * portions[0] // sum(portions)))
    least = 1 if total - largest >= number_of - 1 else 0
    counts, spare = [largest] + [least] * (number_of - 1), total - largest - least * (number_of - 1)
    while spare > 0:
        free = [i for i in range(1, number_of) if counts[i] < largest] or [i for i in range(1, number_of) if counts[i] < reach]
        pool, remaining = sum([portions[i] for i in free]), spare
        for i in free:
            more = min(reach - counts[i], max(1, remaining * portions[i] // pool), spare)
            counts[i] = counts[i] + more
            spare = spare - more
    return np.array(counts)


def scatter_about(own_key, extent, scale, bound, cuts=(), kind=jnp.bfloat16):
    level = shard_levels(own_key, extent, cuts, -0.22, 0.18) if cuts else 1.0
    array = jax.random.normal(own_key, extent, jnp.float32) * scale * level
    return jnp.minimum(jnp.maximum(array, -bound), bound).astype(kind)


def setup_inputs(seed: int = 0) -> dict:
    streams_of = jax.random.split(jax.random.key(seed), 20)
    mixer_input_rows = scatter_about(streams_of[0], (SEQ, D), 1.0, 6.0, ((0, 32),))
    mixer_norm_gain = jnp.clip(1.0 + 0.18 * jax.random.normal(streams_of[1], (D,), jnp.float32), 0.1, 1.9)
    query_weight = scatter_about(streams_of[2], (D, HEADS * HEAD), D ** -0.5, 0.125, ((1, 8),))
    key_weight = scatter_about(streams_of[3], (D, HEADS * HEAD), D ** -0.5, 0.125, ((1, 8),))
    value_weight = scatter_about(streams_of[4], (D, HEADS * HEAD), D ** -0.5, 0.125, ((1, 8),))
    write_strength_projection = scatter_about(streams_of[5], (D, HEADS), D ** -0.5, 0.125)
    decay_projection = scatter_about(streams_of[6], (D, HEADS), D ** -0.5, 0.125)
    head_decay_speed = draw_head_decay_speed(jax.random.fold_in(streams_of[19], 71), 0)
    largest_write_strength = draw_largest_write_strength(jax.random.fold_in(streams_of[19], 71), 0)
    extra_log_decay = draw_extra_log_decay(jax.random.fold_in(streams_of[19], 71), 0)
    head_norm_gain = jnp.clip(1.0 + 0.18 * jax.random.normal(streams_of[10], (HEAD,), jnp.float32), 0.1, 1.9)
    mixer_output_weight = scatter_about(streams_of[11], (HEADS * HEAD, D), (HEADS * HEAD) ** -0.5, 0.125, ((0, 8),))
    expert_input_rows = scatter_about(streams_of[12], (EXP_TOKENS, D), 1.0, 6.0, ((0, 32),))
    expert_norm_gain = jnp.clip(1.0 + 0.18 * jax.random.normal(streams_of[13], (D,), jnp.float32), 0.1, 1.9)
    routes_keys = jax.random.split(jax.random.fold_in(streams_of[14], 1), EXP_TOKENS // EXP_TOK_DEV)
    routes_turns = jax.random.permutation(jax.random.fold_in(streams_of[14], 3), EXP_TOKENS // EXP_TOK_DEV)
    routes = jax.vmap(lambda own, number: routed_block(jax.random.fold_in(streams_of[14], 2), own, number, EXP_TOK_DEV, EXPERTS, TOP, CAP, 2))(routes_keys, routes_turns).reshape((EXP_TOKENS, TOP))
    expert_route_weight = jnp.clip(0.2 + 0.8 * jax.random.uniform(streams_of[15], (EXP_TOKENS, TOP), jnp.float32) ** shard_levels(streams_of[15], (EXP_TOKENS, TOP), ((0, 32),), -0.2, 0.2), 0.2, 1.0)
    gate_weight = scatter_about(streams_of[16], (EXPERTS, D, FF), D ** -0.5, 0.125, ((0, 4), (2, 8)))
    up_weight = scatter_about(streams_of[17], (EXPERTS, D, FF), D ** -0.5, 0.125, ((0, 4), (2, 8)))
    down_weight = scatter_about(streams_of[18], (EXPERTS, FF, D), FF ** -0.5, 0.0625, ((0, 4), (1, 8)))
    return {"mixer_input_rows": mixer_input_rows, "mixer_norm_gain": mixer_norm_gain, "query_weight": query_weight, "key_weight": key_weight, "value_weight": value_weight, "write_strength_projection": write_strength_projection, "decay_projection": decay_projection, "head_decay_speed": head_decay_speed, "largest_write_strength": largest_write_strength, "extra_log_decay": extra_log_decay, "head_norm_gain": head_norm_gain, "mixer_output_weight": mixer_output_weight, "expert_input_rows": expert_input_rows, "expert_norm_gain": expert_norm_gain, "routes": routes, "expert_route_weight": expert_route_weight, "gate_weight": gate_weight, "up_weight": up_weight, "down_weight": down_weight}


norm_eps = 1e-06
highest = lax.Precision.HIGHEST

def rms_scale(rows_in, gain_vec):
    widened = rows_in.astype(jnp.float32)
    scaled = widened * lax.rsqrt(lax.optimization_barrier(jnp.mean(widened * widened, axis=-1, keepdims=True)) + norm_eps)
    return (scaled * gain_vec).astype(jnp.bfloat16)

def unit_rows(tensor):
    return tensor * lax.rsqrt(lax.optimization_barrier(jnp.sum(tensor * tensor, axis=-1, keepdims=True)) + 1e-06)

def block_terms(queries, key_rows, values, log_decay_values, strength):
    length = log_decay_values.shape[-1]
    cumulative = jnp.cumsum(log_decay_values, axis=-1)
    causal = jnp.tril(jnp.ones((length, length), jnp.bool_))
    strict = jnp.tril(jnp.ones((length, length), jnp.bool_), -1)
    decays = jnp.exp(jnp.where(causal, cumulative[..., :, None] - cumulative[..., None, :], -jnp.inf))
    keys_scaled = key_rows * strength[..., None]
    inner_prod = jnp.einsum('...cd,...sd->...cs', keys_scaled, key_rows, precision=highest)
    system = jnp.where(strict, inner_prod * decays, 0.0) + jnp.eye(length, dtype=key_rows.dtype)
    right_side = jnp.concatenate([values * strength[..., None], keys_scaled * jnp.exp(cumulative)[..., None]], axis=-1)
    solved = jax.scipy.linalg.solve_triangular(system, right_side, lower=True, unit_diagonal=True)
    value_width = values.shape[-1]
    carried = solved[..., :value_width]
    weights = solved[..., value_width:]
    scores = jnp.einsum('...cd,...sd->...cs', queries, key_rows, precision=highest) * decays
    query_dec = queries * jnp.exp(cumulative)[..., None]
    keys_dec = key_rows * jnp.exp(cumulative[..., -1:] - cumulative)[..., None]
    last_decay = jnp.exp(cumulative[..., -1])
    return (carried, weights, scores, query_dec, keys_dec, last_decay)

def apply_block(memory, carried, weights, scores, query_dec, keys_dec, last_decay):
    fresh_values = carried - jnp.einsum('...cd,...de->...ce', weights, memory, precision=highest)
    output = jnp.einsum('...cd,...de->...ce', query_dec, memory, precision=highest)
    output = output + jnp.einsum('...cs,...se->...ce', scores, fresh_values, precision=highest)
    memory = memory * last_decay[..., None, None] + jnp.einsum('...cd,...ce->...de', keys_dec, fresh_values, precision=highest)
    return (memory, output)

def reference(mixer_input_rows, mixer_norm_gain, query_weight, key_weight, value_weight, write_strength_projection, decay_projection, head_decay_speed, largest_write_strength, extra_log_decay, head_norm_gain, mixer_output_weight, expert_input_rows, expert_norm_gain, routes, expert_route_weight, gate_weight, up_weight, down_weight):
    mix_normed = rms_scale(mixer_input_rows, mixer_norm_gain)

    def apply_projection(weight):
        return jnp.dot(mix_normed.astype(jnp.float32), weight.astype(jnp.float32), preferred_element_type=jnp.float32)
    queries = jax.nn.silu(apply_projection(query_weight)).reshape(SEQ, HEADS, HEAD)
    key_rows = unit_rows(jax.nn.silu(apply_projection(key_weight)).reshape(SEQ, HEADS, HEAD))
    values = jax.nn.silu(apply_projection(value_weight)).reshape(SEQ, HEADS, HEAD)
    strength = largest_write_strength * jax.nn.sigmoid(apply_projection(write_strength_projection))
    log_decay_values = extra_log_decay - head_decay_speed * jax.nn.softplus(apply_projection(decay_projection))
    block_count = SEQ // BLOCK

    def blocked(tensor):
        return tensor.reshape(block_count, BLOCK, HEADS, -1).transpose(0, 2, 1, 3)

    def advance(memory, pieces):
        return apply_block(memory, *block_terms(*pieces))
    initial = jnp.zeros((HEADS, HEAD, HEAD), jnp.float32)
    _, outputs = lax.scan(advance, initial, (blocked(queries), blocked(key_rows), blocked(values), blocked(log_decay_values[..., None])[..., 0], blocked(strength[..., None])[..., 0]))
    heads_out = outputs.transpose(0, 2, 1, 3).reshape(SEQ, HEADS, HEAD)
    head_outputs_mixed = heads_out * lax.rsqrt(lax.optimization_barrier(jnp.mean(heads_out * heads_out, axis=-1, keepdims=True)) + norm_eps)
    head_outputs_mixed = (head_outputs_mixed * head_norm_gain).reshape(SEQ, HEADS * HEAD).astype(jnp.bfloat16)
    group_width = HEADS_DEV * HEAD

    def add_group(running, group_index):
        columns = lax.dynamic_slice_in_dim(head_outputs_mixed, group_index * group_width, group_width, 1)
        weight_rows = lax.dynamic_slice_in_dim(mixer_output_weight, group_index * group_width, group_width, 0)
        partial_value = jnp.dot(columns.astype(jnp.float32), weight_rows.astype(jnp.float32), preferred_element_type=jnp.float32).astype(jnp.bfloat16)
        return (running + lax.optimization_barrier(partial_value).astype(jnp.float32), None)
    mix_total, _ = lax.scan(add_group, jnp.zeros((SEQ, D), jnp.float32), jnp.arange(N_TP, dtype=jnp.int32))
    mix_out = mix_total.astype(jnp.bfloat16)
    exp_normed = rms_scale(expert_input_rows, expert_norm_gain)
    assigned = routes.reshape(-1)
    shares = expert_route_weight.reshape(-1)
    owners = (jnp.arange(EXP_TOKENS * TOP, dtype=jnp.int32) // TOP).astype(jnp.int32)
    most_rows = N_EP * N_TP * CAP

    def expert_pass(running, expert):
        chosen = assigned == expert
        filled = jnp.sum(chosen.astype(jnp.int32))
        picked = jnp.nonzero(chosen, size=most_rows, fill_value=0)[0].astype(jnp.int32)
        live_rows = jnp.arange(most_rows, dtype=jnp.int32) < filled
        token_ids = owners[picked]
        rows_in = exp_normed[token_ids]
        gate_part = jnp.dot(rows_in.astype(jnp.float32), gate_weight[expert].astype(jnp.float32), preferred_element_type=jnp.float32)
        up_part = jnp.dot(rows_in.astype(jnp.float32), up_weight[expert].astype(jnp.float32), preferred_element_type=jnp.float32)
        hidden = (jax.nn.silu(gate_part) * up_part).astype(jnp.bfloat16)
        pieces = jnp.einsum('rgf,gfd->grd', hidden.reshape(most_rows, N_TP, FF_DEV).astype(jnp.float32), down_weight[expert].reshape(N_TP, FF_DEV, D).astype(jnp.float32))
        rounded = lax.optimization_barrier(pieces.astype(jnp.bfloat16)).astype(jnp.float32)
        expert_rows = lax.optimization_barrier(lax.optimization_barrier(jnp.sum(rounded, axis=0)).astype(jnp.bfloat16)).astype(jnp.float32)
        weight_col = jnp.where(live_rows, shares[picked], 0.0)
        return (running.at[token_ids].add(weight_col[:, None] * expert_rows), None)
    exp_total, _ = lax.scan(expert_pass, jnp.zeros((EXP_TOKENS, D), jnp.float32), jnp.arange(EXPERTS, dtype=jnp.int32))
    return (mix_out, exp_total.astype(jnp.bfloat16))
```

```python
import functools

import jax
import jax.numpy as jnp
from jax import lax
from jax.experimental import pallas as pl
from jax.experimental.pallas import tpu as pltpu
from jax.sharding import PartitionSpec as P

HEAD = 128
BLOCK = 128
CORES = 2

norm_eps = 1e-06
highest = lax.Precision.HIGHEST
f32 = jnp.float32
bf16 = jnp.bfloat16


def narrow(x):
    return x.astype(bf16)


def halves(x):
    top = narrow(x)
    return top, narrow(x - top.astype(f32))


def mm(a, b):
    return jnp.dot(a, b, preferred_element_type=f32)


def mm_nt(a, b):
    return lax.dot_general(a, b, (((1,), (1,)), ((), ())), preferred_element_type=f32)


def square_full(a, b):
    a_top, a_low = halves(a)
    b_top, b_low = halves(b)
    wide = jnp.concatenate([b_top, b_low], axis=1)
    both = mm(
        jnp.concatenate([a_top, a_low], axis=1), jnp.concatenate([wide, wide], axis=0)
    )
    return both[:, : b.shape[1]] + both[:, b.shape[1] :]


def wide_full(a, b):
    a_top, a_low = halves(a)
    b_top, b_low = halves(b)
    return mm(
        jnp.concatenate([a_top, a_low], axis=1), jnp.concatenate([b_top, b_top], axis=0)
    ) + mm(a_top, b_low)


def silu(x):
    return x / (1.0 + jnp.exp(-x))


def rms_rows(rows, gain):
    wide = rows.astype(f32)
    return wide * lax.rsqrt(jnp.mean(wide * wide, axis=-1, keepdims=True) + norm_eps) * gain


def fused_kernel(
    sizes,
    x_ref,
    xgain_ref,
    w8_ref,
    prm_ref,
    extra_ref,
    hgain_ref,
    tok_ref,
    tgain_ref,
    share_ref,
    wq_hbm,
    wk_hbm,
    wv_hbm,
    wo_hbm,
    wg_hbm,
    wu_hbm,
    wd_hbm,
    mix_ref,
    exp_ref,
    wq_ref,
    wk_ref,
    wv_ref,
    wg_ref,
    wu_ref,
    wd_ref,
    rows_all,
    wo_all,
    tok_all,
    part_all,
    part_in,
    line_all,
    line_in,
    own_all,
    query_all,
    pair_all,
    prefix_all,
    run_ref,
    span_out,
    span_in,
    memory_ref,
    mixed_all,
    mixed_in,
    local_sem,
    r_s,
    r_r,
    rs_s,
    rs_r,
    w_s,
    w_r,
    wx_s,
    wx_r,
    ws_s,
    ws_r,
    t_s,
    t_r,
    te_s,
    te_r,
    ts_s,
    ts_r,
    st_s,
    st_r,
    p_s,
    p_r,
    l_s,
    l_r,
    a_s,
    a_r,
):
    EP, Z, H = sizes
    T = Z * CORES
    e = lax.axis_index("ep")
    t = lax.axis_index("tp")
    z = t // CORES
    c = t % CORES
    width = H * HEAD
    model = x_ref.shape[1]
    piece = model // EP
    half = model // 2
    hp = w8_ref.shape[0] // 2

    def remote(src, dst, s, r, **where):
        return pltpu.make_async_remote_copy(
            src_ref=src,
            dst_ref=dst,
            send_sem=s,
            recv_sem=r,
            device_id=where,
            device_id_type=pl.DeviceIdType.MESH,
        )

    def start(copy):
        copy.start()

    def done_send(copy):
        copy.wait_send()

    def done_recv(copy):
        copy.wait_recv()

    def row_copy(zz, step):
        slot = rows_all.at[zz, c]
        d = 0 if step > 0 else 1
        return remote(slot, slot, r_s.at[d, zz], r_r.at[zz], tp=t + step * CORES)

    def row_sibling(zz, core):
        slot = rows_all.at[zz, core]
        return remote(slot, slot, rs_s.at[zz], rs_r.at[zz], tp=z * CORES + 1 - c)

    def wo_slot(zz, core, ee):
        return wo_all.at[zz, core, :, pl.ds(pl.multiple_of(ee * piece, piece), piece)]

    def wo_copy(zz, step):
        slot = wo_slot(zz, c, e)
        d = 0 if step > 0 else 1
        return remote(slot, slot, w_s.at[d, zz], w_r.at[zz], tp=t + step * CORES)

    def wo_peer(zz, frm, to):
        slot = wo_slot(zz, c, frm)
        return remote(slot, slot, wx_s.at[zz, to], wx_r.at[zz, frm], ep=to)

    def wo_sibling(zz, core):
        slot = wo_all.at[zz, core]
        return remote(slot, slot, ws_s.at[zz], ws_r.at[zz], tp=z * CORES + 1 - c)

    def tok_copy(frm, to):
        slot = tok_all.at[e, c, frm]
        return remote(slot, slot, t_s.at[to], t_r.at[frm], tp=to * CORES + c)

    def tok_peer(frm, to):
        slot = tok_all.at[frm, c]
        return remote(slot, slot, te_s.at[to], te_r.at[frm], ep=to)

    def tok_sibling(ee, core):
        slot = tok_all.at[ee, core]
        return remote(slot, slot, ts_s.at[ee], ts_r.at[ee], tp=z * CORES + 1 - c)

    def state_copy(frm, to):
        return remote(span_out, span_in.at[frm], st_s.at[to], st_r.at[frm], ep=to)

    def part_copy(frm, to):
        return remote(part_all.at[to], part_in.at[frm], p_s.at[to], p_r.at[frm], ep=to)

    def line_copy(frm, to):
        return remote(
            line_all.at[to % CORES, to // CORES],
            line_in.at[frm],
            l_s.at[to],
            l_r.at[frm],
            tp=to,
        )

    def mixed_slot(frm):
        return mixed_in.at[:, pl.ds(pl.multiple_of(frm * width, HEAD), width)]

    def mixed_copy(frm, to):
        return remote(mixed_all.at[to], mixed_slot(frm), a_s.at[to], a_r.at[frm], tp=to)

    def eps(other, act):
        for ee in range(EP):
            pl.when(other(ee))(functools.partial(act, ee))

    def tps(act):
        for tt in range(T):
            pl.when(t != tt)(functools.partial(act, tt))

    def zs(act):
        for zz in range(Z):
            pl.when(z != zz)(functools.partial(act, zz))

    others = lambda ee: e != ee

    loads = [
        pltpu.make_async_copy(src, dst, local_sem.at[i])
        for i, (src, dst) in enumerate(
            [
                (wq_hbm, wq_ref),
                (wk_hbm, wk_ref),
                (wv_hbm, wv_ref),
                (wo_hbm, wo_all.at[z, c]),
                (wg_hbm.at[0], wg_ref),
                (wu_hbm.at[0], wu_ref),
                (wd_hbm.at[0], wd_ref),
            ]
        )
    ]
    for load in loads:
        load.start()

    barrier = pltpu.get_barrier_semaphore()

    def greet_tp(tt):
        pl.semaphore_signal(barrier, inc=1, device_id={"tp": tt}, device_id_type=pl.DeviceIdType.MESH)

    def greet_ep(ee):
        pl.semaphore_signal(barrier, inc=1, device_id={"ep": ee}, device_id_type=pl.DeviceIdType.MESH)

    tps(greet_tp)
    eps(others, greet_ep)

    rows_all[z, c] = narrow(rms_rows(x_ref[...], xgain_ref[...]))
    tokens = rms_rows(tok_ref[...], tgain_ref[...])
    share = share_ref[...]
    share_top = narrow(share).astype(f32)
    tok_all[e, c, z] = narrow(
        jnp.concatenate(
            [
                jnp.concatenate([tokens[:, :half], share_top], axis=1),
                jnp.concatenate([tokens[:, half:], share - share_top], axis=1),
            ],
            axis=0,
        )
    )
    pl.semaphore_wait(barrier, T - 1 + EP - 1)

    zs(lambda zz: start(tok_copy(z, zz)))

    def row_forward(zz):
        pl.when((zz <= z) & (z + 1 < Z))(lambda: start(row_copy(zz, 1)))
        pl.when((zz >= z) & (z >= 1))(lambda: start(row_copy(zz, -1)))
        start(row_sibling(zz, c))

    def row_arrive(zz):
        done_recv(row_copy(zz, 1))
        row_forward(zz)

    def wo_forward(zz):
        pl.when((zz <= z) & (z + 1 < Z))(lambda: start(wo_copy(zz, 1)))
        pl.when((zz >= z) & (z >= 1))(lambda: start(wo_copy(zz, -1)))

    def wo_arrive(zz):
        done_recv(wo_copy(zz, 1))
        wo_forward(zz)
        eps(others, lambda ee: start(wo_peer(zz, e, ee)))

    def wo_collect(zz):
        eps(others, lambda ee: done_recv(wo_peer(zz, ee, ee)))
        start(wo_sibling(zz, c))

    def both_sides(s, act):
        pl.when(z - s >= 0)(lambda: act(z - s))
        pl.when(z + s < Z)(lambda: act(z + s))

    for load in loads[:4]:
        load.wait()

    row = lax.broadcasted_iota(jnp.int32, (BLOCK, BLOCK), 0)
    col = lax.broadcasted_iota(jnp.int32, (BLOCK, BLOCK), 1)

    def process(zz):
        causal = row >= col
        strict = row > col
        eye = (row == col).astype(f32)
        upper = (row <= col).astype(f32)
        rows = rows_all[zz].reshape(CORES * BLOCK, model)
        q_all = silu(mm(rows, wq_ref[...]))
        k_all = silu(mm(rows, wk_ref[...]))
        v_all = silu(mm(rows, wv_ref[...]))
        small = mm_nt(w8_ref[...], rows)
        at_rows = pl.ds(pl.multiple_of(zz * CORES * BLOCK, CORES * BLOCK), CORES * BLOCK)
        scale = prm_ref[:, :1]
        strength_rows = scale / (1.0 + jnp.exp(-small))
        softplus = jnp.maximum(small, 0.0) + jnp.log1p(jnp.exp(-jnp.abs(small)))
        decay_rows = extra_ref[:, at_rows] - scale * softplus
        chains = []
        for b in range(CORES):
            at = slice(b * BLOCK, (b + 1) * BLOCK)
            across = jnp.dot(
                decay_rows[:, at], upper, preferred_element_type=f32, precision=highest
            )
            cumulative = across.T
            betas = strength_rows[:, at].T
            for h in range(H):
                of = slice(h * HEAD, (h + 1) * HEAD)
                g = hp + h
                cc = cumulative[:, g : g + 1]
                k = k_all[at, of]
                k = k * lax.rsqrt(jnp.sum(k * k, axis=1, keepdims=True) + 1e-06)
                decays = jnp.exp(jnp.where(causal, cc - across[g : g + 1, :], -1e30))
                chains.append(
                    dict(
                        b=b,
                        h=h,
                        q=q_all[at, of],
                        k=k,
                        v=v_all[at, of],
                        beta=betas[:, h : h + 1],
                        c=cc,
                        decays=decays,
                        last=cumulative[BLOCK - 1 : BLOCK, g : g + 1],
                    )
                )
        for m in chains:
            m["kt"] = m["k"].T
        for m in chains:
            inner = square_full(m["k"], m["kt"])
            m["low"] = jnp.where(strict, inner * m["decays"] * m["beta"], 0.0)
            m["scores"] = narrow(mm(narrow(m["q"]), narrow(m["kt"])) * m["decays"])
        pair_mask = strict & (row // 2 == col // 2)
        for m in chains:
            m["inv"] = eye - jnp.where(pair_mask, m["low"], 0.0)
        size = 2
        while size < BLOCK:
            mask = (row // (2 * size) == col // (2 * size)) & (row // size > col // size)
            for m in chains:
                m["tmp"] = square_full(jnp.where(mask, m["low"], 0.0), m["inv"])
            for m in chains:
                m["inv"] = m["inv"] - square_full(m["inv"], m["tmp"])
            size *= 2
        for m in chains:
            grown = jnp.exp(m["c"])
            m["grown"] = grown
            right = jnp.concatenate(
                [m["v"] * m["beta"], m["k"] * (m["beta"] * grown)], axis=1
            )
            m["solved"] = wide_full(m["inv"], right)
        for m in chains:
            keys_dec_t = (m["k"] * jnp.exp(m["last"] - m["c"])).T
            moved = wide_full(keys_dec_t, m["solved"])
            m["shift"] = moved[:, :HEAD]
            m["map"] = eye * jnp.exp(m["last"]) - moved[:, HEAD:]
            read = mm(m["scores"], narrow(m["solved"]))
            m["own"] = read[:, :HEAD]
            m["query"] = m["q"] * m["grown"] - read[:, HEAD:]
        state = [None] * H
        for m in chains:
            b, h = m["b"], m["h"]
            at, of = slice(b * BLOCK, (b + 1) * BLOCK), slice(h * HEAD, (h + 1) * HEAD)
            if state[h] is None:
                own_all[zz, at, of] = m["own"]
                query_all[zz, at, of] = narrow(m["query"])
                state[h] = jnp.concatenate([m["shift"], m["map"]], axis=1)
            else:
                out = mm(narrow(m["query"]), narrow(state[h]))
                own_all[zz, at, of] = out[:, :HEAD] + m["own"]
                query_all[zz, at, of] = narrow(out[:, HEAD:])
                later = wide_full(m["map"], state[h])
                state[h] = jnp.concatenate(
                    [later[:, :HEAD] + m["shift"], later[:, HEAD:]], axis=1
                )
        for h in range(H):
            pair_all[zz, h] = state[h]

    lines = max(1, min(EP, (2 * BLOCK) // (8 * T)))

    def experts():
        for load in loads[4:]:
            load.wait()
        eps(lambda ee: e >= 0, lambda ee: done_recv(tok_sibling(ee, 1 - c)))
        lane = lax.broadcasted_iota(jnp.int32, (lines * T, 16, HEAD), 2)

        def chunk(i, _):
            span = pl.ds(i * lines, lines)
            got = tok_all[span].reshape(lines * T, 16, half + HEAD).astype(f32)
            count = lines * T * 8
            rows = narrow(
                jnp.concatenate(
                    [
                        got[:, :8, :half].reshape(count, half),
                        got[:, 8:, :half].reshape(count, half),
                    ],
                    axis=1,
                )
            )
            weigh = jnp.sum(
                jnp.where(lane == e, got[:, :, half:], 0.0), axis=2, keepdims=True
            )
            weigh = (weigh[:, :8] + weigh[:, 8:]).reshape(count, 1)
            hidden = narrow(silu(mm(rows, wg_ref[...])) * mm(rows, wu_ref[...]))
            partial = (mm(hidden, wd_ref[...]) * weigh).reshape(lines * T, 8, model)
            part_all[span] = narrow(
                jnp.concatenate([partial[:, :, :half], partial[:, :, half:]], axis=1)
            ).reshape(lines, CORES, Z, 16, half)
            return 0

        lax.fori_loop(0, EP // lines, chunk, 0)

    mid = min(2, Z - 1)

    def step(s, _):
        @pl.when(s == 0)
        def _():
            row_forward(z)

        @pl.when(s >= 1)
        def _():
            both_sides(s, row_arrive)

        @pl.when(s == 1)
        def _():
            wo_forward(z)
            start(wo_sibling(z, c))
            zs(lambda zz: done_recv(tok_copy(zz, zz)))
            eps(others, lambda ee: start(tok_peer(e, ee)))

        @pl.when(s >= 2)
        def _():
            both_sides(s - 1, wo_arrive)

        @pl.when(s == mid)
        def _():
            eps(others, lambda ee: done_recv(tok_peer(ee, ee)))
            eps(lambda ee: e >= 0, lambda ee: start(tok_sibling(ee, c)))

        def side(d, _):
            zz = jnp.where(d == 0, z - s, z + s)

            @pl.when((zz >= 0) & (zz < Z) & ((s > 0) | (d == 0)))
            def _():
                done_recv(row_sibling(zz, 1 - c))
                process(zz)

            return 0

        lax.fori_loop(0, 2, side, 0)

        pl.when(s == max(mid, Z - 2))(experts)
        return 0

    lax.fori_loop(0, Z, step, 0)

    for h in range(H):
        run_ref[h] = pair_all[0, h]

    def compose(zz, _):
        for h in range(H):
            now = run_ref[h]
            prefix_all[zz, h] = narrow(now)
            mine = pair_all[zz, h]
            later = wide_full(mine[:, HEAD:], now)
            run_ref[h] = jnp.concatenate(
                [later[:, :HEAD] + mine[:, :HEAD], later[:, HEAD:]], axis=1
            )
        return 0

    lax.fori_loop(1, Z, compose, 0)
    for h in range(H):
        span_out[h] = narrow(run_ref[h])
    eps(lambda ee: e < ee, lambda ee: start(state_copy(e, ee)))
    eps(others, lambda ee: start(part_copy(e, ee)))
    both_sides(Z - 1, wo_arrive)
    for s in range(1, Z - 1):
        both_sides(s, wo_collect)

    def extend(zz, _):
        for h in range(H):
            of = slice(h * HEAD, (h + 1) * HEAD)
            out = mm(query_all[zz, :, of], prefix_all[zz, h])
            own_all[zz, :, of] += out[:, :HEAD]
            query_all[zz, :, of] = narrow(out[:, HEAD:])
        return 0

    lax.fori_loop(1, Z, extend, 0)

    memory_ref[...] = jnp.zeros_like(memory_ref)

    def enter(ee):
        done_recv(state_copy(ee, ee))
        for h in range(H):
            top, low = halves(memory_ref[h])
            theirs = span_in[ee, h]
            span_map = theirs[:, HEAD:]
            memory_ref[h] = (
                theirs[:, :HEAD].astype(f32) + mm(span_map, top) + mm(span_map, low)
            )

    for ee in range(EP - 1):
        pl.when(ee < e)(functools.partial(enter, ee))

    def finish(zz, _):
        for h in range(H):
            of = slice(h * HEAD, (h + 1) * HEAD)
            top, low = halves(memory_ref[h])
            both = mm(query_all[zz, :, of], jnp.concatenate([top, low], axis=1))
            heads = own_all[zz, :, of] + both[:, :HEAD] + both[:, HEAD:]
            scale = lax.rsqrt(jnp.mean(heads * heads, axis=1, keepdims=True) + norm_eps)
            done = narrow(heads * scale * hgain_ref[...])
            for b in range(CORES):
                mixed_all[zz * CORES + b, :, of] = done[b * BLOCK : (b + 1) * BLOCK]
        return 0

    lax.fori_loop(0, Z, finish, 0)
    tps(lambda tt: start(mixed_copy(t, tt)))
    mine = pltpu.make_async_copy(mixed_all.at[t], mixed_slot(t), local_sem.at[7])
    mine.start()

    total = part_all[e].astype(f32)
    part_in[e] = jnp.zeros_like(part_in[e])
    eps(others, lambda ee: done_recv(part_copy(ee, ee)))
    for ee in range(EP):
        total = total + part_in[ee].astype(f32)
    line_all[...] = narrow(total)
    line_in[t] = line_all[c, z]
    tps(lambda tt: start(line_copy(t, tt)))

    both_sides(Z - 1, wo_collect)
    zs(lambda zz: done_recv(wo_sibling(zz, 1 - c)))
    done_recv(wo_sibling(z, 1 - c))
    mine.wait()
    tps(lambda tt: done_recv(mixed_copy(tt, tt)))
    tile = min(512, model)

    def project(i, _):
        at = pl.ds(pl.multiple_of(i * tile, tile), tile)
        mix_ref[:, at] = narrow(
            mm(mixed_in[...], wo_all[:, :, :, at].reshape(T * width, tile))
        )
        return 0

    lax.fori_loop(0, model // tile, project, 0)

    tps(lambda tt: done_recv(line_copy(tt, tt)))
    result = jnp.zeros((16, half), f32)
    for tt in range(T):
        result = result + line_in[tt].astype(f32)
    exp_ref[...] = narrow(jnp.concatenate([result[:8], result[8:]], axis=1))

    zs(lambda zz: done_send(tok_copy(z, zz)))

    def drain(zz, _):
        for copy in (row_copy, wo_copy):
            pl.when((zz <= z) & (z + 1 < Z))(lambda: done_send(copy(zz, 1)))
            pl.when((zz >= z) & (z >= 1))(lambda: done_send(copy(zz, -1)))
        done_send(row_sibling(zz, c))
        done_send(wo_sibling(zz, c))

        @pl.when(zz != z)
        def _():
            eps(others, lambda ee: done_send(wo_peer(zz, e, ee)))

        return 0

    lax.fori_loop(0, Z, drain, 0)
    eps(others, lambda ee: done_send(tok_peer(e, ee)))
    eps(lambda ee: e >= 0, lambda ee: done_send(tok_sibling(ee, c)))
    eps(lambda ee: e < ee, lambda ee: done_send(state_copy(e, ee)))
    eps(others, lambda ee: done_send(part_copy(e, ee)))
    tps(lambda tt: done_send(line_copy(t, tt)))
    tps(lambda tt: done_send(mixed_copy(t, tt)))


def body(
    mixer_input_rows,
    mixer_norm_gain,
    query_weight,
    key_weight,
    value_weight,
    write_strength_projection,
    decay_projection,
    head_decay_speed,
    largest_write_strength,
    extra_log_decay,
    head_norm_gain,
    mixer_output_weight,
    expert_input_rows,
    expert_norm_gain,
    routes,
    expert_route_weight,
    gate_weight,
    up_weight,
    down_weight,
):
    EP, T = lax.axis_size("ep"), lax.axis_size("tp")
    Z = T // CORES
    H = head_decay_speed.shape[0]
    hp = 4 * -(-H // 4)
    width = H * HEAD
    block, model = mixer_input_rows.shape
    toks = expert_input_rows.shape[0]
    half = model // 2
    hidden = gate_weight.shape[2]
    first = lax.axis_index("tp") * H
    assert block == BLOCK and toks == 8

    def stack(a, b):
        rest = [(0, 0)] * (a.ndim - 1)
        return jnp.concatenate(
            [jnp.pad(a, [(0, hp - H)] + rest), jnp.pad(b, [(0, hp - H)] + rest)], axis=0
        )

    w8 = stack(
        lax.dynamic_slice_in_dim(write_strength_projection.T, first, H, 0),
        lax.dynamic_slice_in_dim(decay_projection.T, first, H, 0),
    )
    prm = jnp.broadcast_to(
        stack(largest_write_strength, head_decay_speed)[:, None], (2 * hp, HEAD)
    )
    extra = jnp.pad(extra_log_decay.T, ((hp, hp - H), (0, 0)))
    lanes = lax.broadcasted_iota(jnp.int32, (toks, HEAD), 1)
    share = jnp.zeros((toks, HEAD), f32)
    for j in range(routes.shape[1]):
        share = share + jnp.where(
            lanes == routes[:, j : j + 1], expert_route_weight[:, j : j + 1], 0.0
        )

    vmem = pl.BlockSpec(memory_space=pltpu.VMEM)
    anywhere = pl.BlockSpec(memory_space=pl.ANY)
    dma = pltpu.SemaphoreType.DMA
    V = pltpu.VMEM
    return pl.pallas_call(
        functools.partial(fused_kernel, (EP, Z, H)),
        in_specs=[vmem] * 9 + [anywhere] * 7,
        out_specs=[vmem, vmem],
        out_shape=[
            jax.ShapeDtypeStruct((block, model), bf16),
            jax.ShapeDtypeStruct((toks, model), bf16),
        ],
        scratch_shapes=[
            V((model, width), bf16),
            V((model, width), bf16),
            V((model, width), bf16),
            V((model, hidden), bf16),
            V((model, hidden), bf16),
            V((hidden, model), bf16),
            V((Z, CORES, BLOCK, model), bf16),
            V((Z, CORES, width, model), bf16),
            V((EP, CORES, Z, 16, half + HEAD), bf16),
            V((EP, CORES, Z, 16, half), bf16),
            V((EP, CORES, Z, 16, half), bf16),
            V((CORES, Z, 16, half), bf16),
            V((T, 16, half), bf16),
            V((Z, CORES * BLOCK, width), f32),
            V((Z, CORES * BLOCK, width), bf16),
            V((Z, H, HEAD, 2 * HEAD), f32),
            V((Z, H, HEAD, 2 * HEAD), bf16),
            V((H, HEAD, 2 * HEAD), f32),
            V((H, HEAD, 2 * HEAD), bf16),
            V((EP, H, HEAD, 2 * HEAD), bf16),
            V((H, HEAD, HEAD), f32),
            V((T, BLOCK, width), bf16),
            V((BLOCK, T * width), bf16),
            dma((8,)),
            dma((2, Z)),
            dma((Z,)),
            dma((Z,)),
            dma((Z,)),
            dma((2, Z)),
            dma((Z,)),
            dma((Z, EP)),
            dma((Z, EP)),
            dma((Z,)),
            dma((Z,)),
            dma((Z,)),
            dma((Z,)),
            dma((EP,)),
            dma((EP,)),
            dma((EP,)),
            dma((EP,)),
            dma((EP,)),
            dma((EP,)),
            dma((EP,)),
            dma((EP,)),
            dma((T,)),
            dma((T,)),
            dma((T,)),
            dma((T,)),
        ],
        compiler_params=pltpu.CompilerParams(
            collective_id=0, has_side_effects=True, vmem_limit_bytes=60 * 1024 * 1024
        ),
    )(
        mixer_input_rows,
        mixer_norm_gain.reshape(1, model),
        w8,
        prm,
        extra,
        head_norm_gain.reshape(1, HEAD),
        expert_input_rows,
        expert_norm_gain.reshape(1, model),
        share,
        query_weight,
        key_weight,
        value_weight,
        mixer_output_weight,
        gate_weight,
        up_weight,
        down_weight,
    )


def solution(mesh):
    placed = (
        P(("ep", "tp"), None),
        P(),
        P(None, "tp"),
        P(None, "tp"),
        P(None, "tp"),
        P(),
        P(),
        P("tp"),
        P("tp"),
        P("ep", "tp"),
        P(),
        P("tp", None),
        P(("ep", "tp"), None),
        P(),
        P(("ep", "tp"), None),
        P(("ep", "tp"), None),
        P("ep", None, "tp"),
        P("ep", None, "tp"),
        P("ep", "tp", None),
    )
    return jax.shard_map(
        body,
        mesh=mesh,
        in_specs=placed,
        out_specs=(P(("ep", "tp"), None), P(("ep", "tp"), None)),
        check_vma=False,
    )
```

```python
import functools

import jax
import jax.numpy as jnp
from jax import lax
from jax.experimental import pallas as pl
from jax.experimental.pallas import tpu as pltpu
from jax.sharding import PartitionSpec as P

HEAD = 128
BLOCK = 128
CORES = 2

norm_eps = 1e-06
highest = lax.Precision.HIGHEST
f32 = jnp.float32
bf16 = jnp.bfloat16


def narrow(x):
    return x.astype(bf16)


def halves(x):
    top = narrow(x)
    return top, narrow(x - top.astype(f32))


def mm(a, b):
    return jnp.dot(a, b, preferred_element_type=f32)


def mm_nt(a, b):
    return lax.dot_general(a, b, (((1,), (1,)), ((), ())), preferred_element_type=f32)


def square_full(a, b):
    a_top, a_low = halves(a)
    b_top, b_low = halves(b)
    wide = jnp.concatenate([b_top, b_low], axis=1)
    both = mm(
        jnp.concatenate([a_top, a_low], axis=1), jnp.concatenate([wide, wide], axis=0)
    )
    return both[:, : b.shape[1]] + both[:, b.shape[1] :]


def wide_full(a, b):
    a_top, a_low = halves(a)
    b_top, b_low = halves(b)
    return mm(
        jnp.concatenate([a_top, a_low], axis=1), jnp.concatenate([b_top, b_top], axis=0)
    ) + mm(a_top, b_low)


def silu(x):
    return x / (1.0 + jnp.exp(-x))


def rms_rows(rows, gain):
    wide = rows.astype(f32)
    return wide * lax.rsqrt(jnp.mean(wide * wide, axis=-1, keepdims=True) + norm_eps) * gain


def fused_kernel(
    sizes,
    x_ref,
    xgain_ref,
    wst_ref,
    wdt_ref,
    largest_ref,
    speed_ref,
    extra_ref,
    hgain_ref,
    tok_ref,
    tgain_ref,
    routes_ref,
    weigh_ref,
    wq_hbm,
    wk_hbm,
    wv_hbm,
    wo_hbm,
    wg_hbm,
    wu_hbm,
    wd_hbm,
    mix_ref,
    exp_ref,
    wsmall_ref,
    wq_ref,
    wk_ref,
    wv_ref,
    wg_ref,
    wu_ref,
    wd_ref,
    rows_all,
    wo_all,
    tok_all,
    part_all,
    part_sib,
    part_sum,
    part_in,
    line_all,
    line_in,
    own_all,
    query_all,
    pair_all,
    prefix_all,
    run_ref,
    span_out,
    span_in,
    memory_ref,
    total_ref,
    mixed_all,
    mixed_in,
    local_sem,
    r_s,
    r_r,
    rs_s,
    rs_r,
    w_s,
    w_r,
    wx_s,
    wx_r,
    wh_s,
    wh_r,
    ws_s,
    ws_r,
    t_s,
    t_r,
    te_s,
    te_r,
    ts_s,
    ts_r,
    st_s,
    st_r,
    ps_s,
    ps_r,
    p_s,
    p_r,
    l_s,
    l_r,
    a_s,
    a_r,
):
    EP, Z, H = sizes
    T = Z * CORES
    e = lax.axis_index("ep")
    t = lax.axis_index("tp")
    z = t // CORES
    c = t % CORES
    width = H * HEAD
    model = x_ref.shape[1]
    piece = model // EP
    half = model // 2
    hp = 4 * -(-H // 4)
    relayed = EP == 4

    def remote(src, dst, s, r, **where):
        return pltpu.make_async_remote_copy(
            src_ref=src,
            dst_ref=dst,
            send_sem=s,
            recv_sem=r,
            device_id=where,
            device_id_type=pl.DeviceIdType.MESH,
        )

    def start(copy):
        copy.start()

    def done_send(copy):
        copy.wait_send()

    def done_recv(copy):
        copy.wait_recv()

    def row_copy(zz, step):
        slot = rows_all.at[zz, c]
        d = 0 if step > 0 else 1
        return remote(slot, slot, r_s.at[d, zz], r_r.at[zz], tp=t + step * CORES)

    def row_sibling(zz, core):
        slot = rows_all.at[zz, core]
        return remote(slot, slot, rs_s.at[zz], rs_r.at[zz], tp=z * CORES + 1 - c)

    def wo_slot(zz, core, ee):
        return wo_all.at[zz, core, :, pl.ds(pl.multiple_of(ee * piece, piece), piece)]

    def wo_copy(zz, step):
        slot = wo_slot(zz, c, e)
        d = 0 if step > 0 else 1
        return remote(slot, slot, w_s.at[d, zz], w_r.at[zz], tp=t + step * CORES)

    def wo_peer(zz, frm, to):
        slot = wo_slot(zz, c, frm)
        return remote(slot, slot, wx_s.at[zz, to], wx_r.at[zz, frm], ep=to)

    def wo_half(zz, ee, i):
        rows = width // 2
        slot = wo_all.at[
            zz, c, i * rows : (i + 1) * rows, pl.ds(pl.multiple_of(ee * piece, piece), piece)
        ]
        return remote(slot, slot, wh_s.at[zz, i], wh_r.at[zz, i], ep=e ^ (2 - i))

    def wo_sibling(zz, core, ee):
        slot = wo_slot(zz, core, ee)
        return remote(slot, slot, ws_s.at[zz, ee], ws_r.at[zz, ee], tp=z * CORES + 1 - c)

    def wo_siblings(zz, core, act):
        for ee in range(EP):
            act(wo_sibling(zz, core, ee))

    def tok_copy(frm, to):
        slot = tok_all.at[e, c, frm]
        return remote(slot, slot, t_s.at[to], t_r.at[frm], tp=to * CORES + c)

    def tok_peer(frm, to):
        slot = tok_all.at[frm, c]
        return remote(slot, slot, te_s.at[to], te_r.at[frm], ep=to)

    def tok_sibling(ee, core):
        slot = tok_all.at[ee, core]
        return remote(slot, slot, ts_s.at[ee], ts_r.at[ee], tp=z * CORES + 1 - c)

    def state_copy(frm, to, i):
        return remote(
            span_out.at[i], span_in.at[frm, i], st_s.at[to, i], st_r.at[frm, i], ep=to
        )

    def part_sibling():
        return remote(
            part_all.at[1 - c], part_sib, ps_s.at[0], ps_r.at[0], tp=z * CORES + 1 - c
        )

    def part_copy(frm, to):
        return remote(part_sum.at[to], part_in.at[frm], p_s.at[to], p_r.at[frm], ep=to)

    def line_copy(frm, to):
        return remote(
            line_all.at[to], line_in.at[frm], l_s.at[to], l_r.at[frm], tp=to * CORES + c
        )

    def mixed_slot(frm):
        return mixed_in.at[:, pl.ds(pl.multiple_of(frm * width, HEAD), width)]

    def mixed_copy(frm, to):
        return remote(mixed_all.at[to], mixed_slot(frm), a_s.at[to], a_r.at[frm], tp=to)

    def eps(other, act):
        for ee in range(EP):
            pl.when(other(ee))(functools.partial(act, ee))

    def tps(act):
        for tt in range(T):
            pl.when(t != tt)(functools.partial(act, tt))

    def zs(act):
        for zz in range(Z):
            pl.when(z != zz)(functools.partial(act, zz))

    others = lambda ee: e != ee
    peers = (lambda ee: (e ^ 1 == ee) | (e ^ 2 == ee)) if relayed else others

    loads = [
        pltpu.make_async_copy(src, dst, local_sem.at[i])
        for i, (src, dst) in enumerate(
            [
                (wq_hbm, wq_ref),
                (wk_hbm, wk_ref),
                (wv_hbm, wv_ref),
                (wo_hbm, wo_all.at[z, c]),
                (wg_hbm.at[0], wg_ref),
                (wu_hbm.at[0], wu_ref),
                (wd_hbm.at[0], wd_ref),
            ]
        )
    ]

    barrier = pltpu.get_barrier_semaphore()

    def greet_tp(tt):
        pl.semaphore_signal(barrier, inc=1, device_id={"tp": tt}, device_id_type=pl.DeviceIdType.MESH)

    def greet_ep(ee):
        pl.semaphore_signal(barrier, inc=1, device_id={"ep": ee}, device_id_type=pl.DeviceIdType.MESH)

    tps(greet_tp)
    eps(others, greet_ep)
    for load in loads[:4]:
        load.start()

    rows_all[z, c] = narrow(rms_rows(x_ref[...], xgain_ref[...]))
    wsmall_ref[...] = jnp.concatenate([wst_ref[...], wdt_ref[...]], axis=0)
    tokens = rms_rows(tok_ref[...], tgain_ref[...])
    count = tokens.shape[0]
    diagonal = lax.broadcasted_iota(jnp.int32, (count, count), 0) == lax.broadcasted_iota(
        jnp.int32, (count, count), 1
    )
    lanes = lax.broadcasted_iota(jnp.int32, (count, HEAD), 1)
    share = jnp.zeros((count, HEAD), f32)
    for j in range(routes_ref.shape[0]):

        def column(ref):
            line = ref[j : j + 1, :].astype(f32)
            return jnp.sum(jnp.where(diagonal, line, 0.0), axis=1, keepdims=True)

        share = share + jnp.where(lanes.astype(f32) == column(routes_ref), column(weigh_ref), 0.0)
    share_top = narrow(share).astype(f32)
    tok_all[e, c, z] = narrow(
        jnp.concatenate(
            [
                jnp.concatenate([tokens[:, :half], share_top], axis=1),
                jnp.concatenate([tokens[:, half:], share - share_top], axis=1),
            ],
            axis=0,
        )
    )
    pl.semaphore_wait(barrier, T - 1 + EP - 1)

    zs(lambda zz: start(tok_copy(z, zz)))

    def row_forward(zz):
        pl.when((zz <= z) & (z + 1 < Z))(lambda: start(row_copy(zz, 1)))
        pl.when((zz >= z) & (z >= 1))(lambda: start(row_copy(zz, -1)))
        start(row_sibling(zz, c))

    def row_arrive(zz):
        done_recv(row_copy(zz, 1))
        row_forward(zz)

    def wo_forward(zz):
        pl.when((zz <= z) & (z + 1 < Z))(lambda: start(wo_copy(zz, 1)))
        pl.when((zz >= z) & (z >= 1))(lambda: start(wo_copy(zz, -1)))

    def wo_arrive(zz):
        done_recv(wo_copy(zz, 1))
        eps(peers, lambda ee: start(wo_peer(zz, e, ee)))
        start(wo_sibling(zz, c, e))

    def wo_relay(zz):
        if relayed:
            for i in range(2):
                done_recv(wo_peer(zz, e ^ (1 + i), e))
                start(wo_half(zz, e ^ (1 + i), i))
                start(wo_sibling(zz, c, e ^ (1 + i)))

    def wo_collect(zz):
        if relayed:
            for i in range(2):
                done_recv(wo_half(zz, e ^ 3, i))
            start(wo_sibling(zz, c, e ^ 3))
        else:

            def pass_on(ee):
                done_recv(wo_peer(zz, ee, ee))
                start(wo_sibling(zz, c, ee))

            eps(others, pass_on)

    def both_sides(s, act):
        pl.when(z - s >= 0)(lambda: act(z - s))
        pl.when(z + s < Z)(lambda: act(z + s))

    row_forward(z)
    loads[3].wait()
    wo_forward(z)
    wo_siblings(z, c, start)
    for load in loads[4:]:
        load.start()
    for load in loads[:3]:
        load.wait()

    row = lax.broadcasted_iota(jnp.int32, (BLOCK, BLOCK), 0)
    col = lax.broadcasted_iota(jnp.int32, (BLOCK, BLOCK), 1)

    def process(zz):
        causal = row >= col
        strict = row > col
        eye = (row == col).astype(f32)
        upper = (row <= col).astype(f32)
        rows = rows_all[zz].reshape(CORES * BLOCK, model)
        q_all = silu(mm(rows, wq_ref[...]))
        k_all = silu(mm(rows, wk_ref[...]))
        v_all = silu(mm(rows, wv_ref[...]))
        at_rows = pl.ds(pl.multiple_of(zz * CORES * BLOCK, CORES * BLOCK), CORES * BLOCK)
        heads = wst_ref.shape[0]
        every = mm_nt(wsmall_ref[...], rows)
        head = lax.broadcasted_iota(jnp.int32, (2 * heads, CORES * BLOCK), 0)
        place = lax.broadcasted_iota(jnp.int32, (2 * hp, CORES * BLOCK), 0)

        def pick(first):
            return [
                jnp.sum(jnp.where(head == first + t * H + h, every, 0.0), axis=0, keepdims=True)
                for h in range(H)
            ]

        def tiled(lines, first):
            out = jnp.zeros((2 * hp, CORES * BLOCK), f32)
            for h, line in enumerate(lines):
                out = jnp.where(place == first + h, line, out)
            return out

        strength_rows = tiled(
            [
                largest_ref[:, h : h + 1] / (1.0 + jnp.exp(-v))
                for h, v in enumerate(pick(0))
            ],
            0,
        )
        decay_rows = tiled(
            [
                extra_ref[h : h + 1, at_rows]
                - speed_ref[:, h : h + 1]
                * (jnp.maximum(v, 0.0) + jnp.log1p(jnp.exp(-jnp.abs(v))))
                for h, v in enumerate(pick(heads))
            ],
            hp,
        )
        chains = []
        for b in range(CORES):
            at = slice(b * BLOCK, (b + 1) * BLOCK)
            across = jnp.dot(
                decay_rows[:, at], upper, preferred_element_type=f32, precision=highest
            )
            cumulative = across.T
            betas = strength_rows[:, at].T
            for h in range(H):
                of = slice(h * HEAD, (h + 1) * HEAD)
                g = hp + h
                cc = cumulative[:, g : g + 1]
                k = k_all[at, of]
                k = k * lax.rsqrt(jnp.sum(k * k, axis=1, keepdims=True) + 1e-06)
                decays = jnp.exp(jnp.where(causal, cc - across[g : g + 1, :], -1e30))
                chains.append(
                    dict(
                        b=b,
                        h=h,
                        q=q_all[at, of],
                        k=k,
                        v=v_all[at, of],
                        beta=betas[:, h : h + 1],
                        c=cc,
                        decays=decays,
                        last=cumulative[BLOCK - 1 : BLOCK, g : g + 1],
                    )
                )
        for m in chains:
            m["kt"] = m["k"].T
        for m in chains:
            inner = square_full(m["k"], m["kt"])
            m["low"] = jnp.where(strict, inner * m["decays"] * m["beta"], 0.0)
            m["scores"] = narrow(mm(narrow(m["q"]), narrow(m["kt"])) * m["decays"])
        pair_mask = strict & (row // 2 == col // 2)
        for m in chains:
            m["inv"] = eye - jnp.where(pair_mask, m["low"], 0.0)
        size = 2
        while size < BLOCK:
            mask = (row // (2 * size) == col // (2 * size)) & (row // size > col // size)
            for m in chains:
                m["tmp"] = square_full(jnp.where(mask, m["low"], 0.0), m["inv"])
            for m in chains:
                m["inv"] = m["inv"] - square_full(m["inv"], m["tmp"])
            size *= 2
        for m in chains:
            grown = jnp.exp(m["c"])
            m["grown"] = grown
            right = jnp.concatenate(
                [m["v"] * m["beta"], m["k"] * (m["beta"] * grown)], axis=1
            )
            m["solved"] = wide_full(m["inv"], right)
        for m in chains:
            keys_dec_t = (m["k"] * jnp.exp(m["last"] - m["c"])).T
            moved = wide_full(keys_dec_t, m["solved"])
            m["shift"] = moved[:, :HEAD]
            m["map"] = eye * jnp.exp(m["last"]) - moved[:, HEAD:]
            read = mm(m["scores"], narrow(m["solved"]))
            m["own"] = read[:, :HEAD]
            m["query"] = m["q"] * m["grown"] - read[:, HEAD:]
        state = [None] * H
        for m in chains:
            b, h = m["b"], m["h"]
            at, of = slice(b * BLOCK, (b + 1) * BLOCK), slice(h * HEAD, (h + 1) * HEAD)
            if state[h] is None:
                own_all[zz, at, of] = m["own"]
                query_all[zz, at, of] = narrow(m["query"])
                state[h] = jnp.concatenate([m["shift"], m["map"]], axis=1)
            else:
                out = mm(narrow(m["query"]), narrow(state[h]))
                own_all[zz, at, of] = out[:, :HEAD] + m["own"]
                query_all[zz, at, of] = narrow(out[:, HEAD:])
                later = wide_full(m["map"], state[h])
                state[h] = jnp.concatenate(
                    [later[:, :HEAD] + m["shift"], later[:, HEAD:]], axis=1
                )
        for h in range(H):
            pair_all[zz, h] = state[h]

    lines = max(1, min(EP, (2 * BLOCK) // (8 * T)))

    def experts():
        for load in loads[4:]:
            load.wait()
        eps(lambda ee: e >= 0, lambda ee: done_recv(tok_sibling(ee, 1 - c)))
        lane = lax.broadcasted_iota(jnp.int32, (lines * T, 16, HEAD), 2)

        def chunk(i, _):
            span = pl.ds(i * lines, lines)
            got = tok_all[span].reshape(lines * T, 16, half + HEAD).astype(f32)
            count = lines * T * 8
            rows = narrow(
                jnp.concatenate(
                    [
                        got[:, :8, :half].reshape(count, half),
                        got[:, 8:, :half].reshape(count, half),
                    ],
                    axis=1,
                )
            )
            weigh = jnp.sum(
                jnp.where(lane == e, got[:, :, half:], 0.0), axis=2, keepdims=True
            )
            weigh = (weigh[:, :8] + weigh[:, 8:]).reshape(count, 1)
            hidden = narrow(silu(mm(rows, wg_ref[...])) * mm(rows, wu_ref[...]))
            partial = (mm(hidden, wd_ref[...]) * weigh).reshape(lines * T, 8, model)
            both = narrow(
                jnp.concatenate([partial[:, :, :half], partial[:, :, half:]], axis=1)
            ).reshape(lines, CORES, Z, 16, half)
            for core in range(CORES):
                part_all[core, span] = both[:, core]
            return 0

        lax.fori_loop(0, EP // lines, chunk, 0)

    mid, late = min(1, Z - 1), min(2, Z - 1)

    def step(s, _):
        @pl.when(s >= 1)
        def _():
            both_sides(s, row_arrive)

        @pl.when((s >= 2) & (s <= Z - 2))
        def _():
            both_sides(s - 1, wo_forward)

        @pl.when(s == mid)
        def _():
            eps(others, lambda ee: done_recv(tok_peer(ee, ee)))
            eps(lambda ee: e >= 0, lambda ee: start(tok_sibling(ee, c)))

        @pl.when(s == late)
        def _():
            done_recv(part_sibling())
            part_sum[...] = narrow(part_all[c].astype(f32) + part_sib[...].astype(f32))
            eps(others, lambda ee: start(part_copy(e, ee)))

        def side(d, _):
            zz = jnp.where(d == 0, z - s, z + s)

            @pl.when((zz >= 0) & (zz < Z) & ((s > 0) | (d == 0)))
            def _():
                done_recv(row_sibling(zz, 1 - c))
                process(zz)

            return 0

        lax.fori_loop(0, 2, side, 0)

        @pl.when(s == 0)
        def _():
            zs(lambda zz: done_recv(tok_copy(zz, zz)))
            eps(others, lambda ee: start(tok_peer(e, ee)))

        @pl.when((s >= 1) & (s <= Z - 3))
        def _():
            both_sides(s, wo_arrive)

        @pl.when(s == mid)
        def _():
            experts()
            start(part_sibling())

        @pl.when((s >= 2) & (s <= Z - 2))
        def _():
            both_sides(s - 1, wo_relay)

        return 0

    lax.fori_loop(0, Z, step, 0)

    for h in range(H):
        run_ref[h] = pair_all[0, h]

    def compose(zz, _):
        for h in range(H):
            now = run_ref[h]
            prefix_all[zz, h] = narrow(now)
            mine = pair_all[zz, h]
            later = wide_full(mine[:, HEAD:], now)
            run_ref[h] = jnp.concatenate(
                [later[:, :HEAD] + mine[:, :HEAD], later[:, HEAD:]], axis=1
            )
        return 0

    lax.fori_loop(1, Z, compose, 0)
    for h in range(H):
        span_out[0, h] = narrow(run_ref[h, :, :HEAD])
        span_out[1, h] = narrow(run_ref[h, :, HEAD:])
    eps(lambda ee: e < ee, lambda ee: start(state_copy(e, ee, 0)))
    eps(lambda ee: (e < ee) & (e > 0), lambda ee: start(state_copy(e, ee, 1)))
    first_left = max(1, Z - 2)
    if Z >= 2:
        both_sides(first_left, wo_arrive)
        both_sides(first_left, wo_forward)

    def extend(zz, _):
        for h in range(H):
            of = slice(h * HEAD, (h + 1) * HEAD)
            out = mm(query_all[zz, :, of], prefix_all[zz, h])
            own_all[zz, :, of] += out[:, :HEAD]
            query_all[zz, :, of] = narrow(out[:, HEAD:])
        return 0

    lax.fori_loop(1, Z, extend, 0)
    for s in range(1, first_left):
        both_sides(s, wo_collect)

    memory_ref[...] = jnp.zeros_like(memory_ref)

    def enter(ee):
        done_recv(state_copy(ee, ee, 0))
        if ee == 0:
            memory_ref[...] = span_in[0, 0].astype(f32)
            return
        done_recv(state_copy(ee, ee, 1))
        for h in range(H):
            top, low = halves(memory_ref[h])
            span_map = span_in[ee, 1, h]
            memory_ref[h] = (
                span_in[ee, 0, h].astype(f32) + mm(span_map, top) + mm(span_map, low)
            )

    for ee in range(EP - 1):
        pl.when(ee < e)(functools.partial(enter, ee))

    def finish(zz, _):
        for h in range(H):
            of = slice(h * HEAD, (h + 1) * HEAD)
            top, low = halves(memory_ref[h])
            both = mm(query_all[zz, :, of], jnp.concatenate([top, low], axis=1))
            heads = own_all[zz, :, of] + both[:, :HEAD] + both[:, HEAD:]
            scale = lax.rsqrt(jnp.mean(heads * heads, axis=1, keepdims=True) + norm_eps)
            done = narrow(heads * scale * hgain_ref[...])
            for b in range(CORES):
                mixed_all[zz * CORES + b, :, of] = done[b * BLOCK : (b + 1) * BLOCK]
        return 0

    lax.fori_loop(0, Z, finish, 0)
    tps(lambda tt: start(mixed_copy(t, tt)))
    mine = pltpu.make_async_copy(mixed_all.at[t], mixed_slot(t), local_sem.at[7])
    mine.start()
    for s in range(first_left + 1, Z):
        both_sides(s, wo_arrive)
    if Z >= 2:
        both_sides(first_left, wo_relay)

    eps(others, lambda ee: done_recv(part_copy(ee, ee)))
    part_in[e] = part_sum[e]
    total = part_in[0].astype(f32)
    for ee in range(1, EP):
        total = total + part_in[ee].astype(f32)
    line_all[...] = narrow(total)
    line_in[z] = line_all[z]
    zs(lambda zz: start(line_copy(z, zz)))

    def project(zz):
        for b in range(CORES):
            tt = zz * CORES + b
            pl.when(tt != t)(lambda: done_recv(mixed_copy(tt, tt)))
        wo_siblings(zz, 1 - c, done_recv)
        heads = mixed_in[:, pl.ds(pl.multiple_of(zz * CORES * width, HEAD), CORES * width)]
        total_ref[...] += mm(heads, wo_all[zz].reshape(CORES * width, model))

    total_ref[...] = jnp.zeros_like(total_ref)
    for s in range(first_left + 1, Z):
        both_sides(s, wo_relay)
    if Z >= 2:
        both_sides(first_left, wo_collect)
    mine.wait()

    def near(s, _):
        def side(d, _):
            zz = jnp.where(d == 0, z - s, z + s)

            @pl.when((zz >= 0) & (zz < Z) & ((s > 0) | (d == 0)))
            def _():
                @pl.when((s > first_left))
                def _():
                    wo_collect(zz)

                project(zz)

            return 0

        lax.fori_loop(0, 2, side, 0)
        return 0

    lax.fori_loop(0, Z, near, 0)
    mix_ref[...] = narrow(total_ref[...])

    zs(lambda zz: done_recv(line_copy(zz, zz)))
    result = line_in[0].astype(f32)
    for zz in range(1, Z):
        result = result + line_in[zz].astype(f32)
    exp_ref[...] = narrow(jnp.concatenate([result[:8], result[8:]], axis=1))

    zs(lambda zz: done_send(tok_copy(z, zz)))

    def drain(zz, _):
        for copy in (row_copy, wo_copy):
            pl.when((zz <= z) & (z + 1 < Z))(lambda: done_send(copy(zz, 1)))
            pl.when((zz >= z) & (z >= 1))(lambda: done_send(copy(zz, -1)))
        done_send(row_sibling(zz, c))
        wo_siblings(zz, c, done_send)

        @pl.when(zz != z)
        def _():
            eps(peers, lambda ee: done_send(wo_peer(zz, e, ee)))
            if relayed:
                for i in range(2):
                    done_send(wo_half(zz, e ^ (1 + i), i))

        return 0

    lax.fori_loop(0, Z, drain, 0)
    eps(others, lambda ee: done_send(tok_peer(e, ee)))
    eps(lambda ee: e >= 0, lambda ee: done_send(tok_sibling(ee, c)))
    eps(lambda ee: e < ee, lambda ee: done_send(state_copy(e, ee, 0)))
    eps(lambda ee: (e < ee) & (e > 0), lambda ee: done_send(state_copy(e, ee, 1)))
    eps(others, lambda ee: done_send(part_copy(e, ee)))
    done_send(part_sibling())
    zs(lambda zz: done_send(line_copy(z, zz)))
    tps(lambda tt: done_send(mixed_copy(t, tt)))


def body(
    mixer_input_rows,
    mixer_norm_gain,
    query_weight,
    key_weight,
    value_weight,
    write_strength_projection,
    decay_projection,
    head_decay_speed,
    largest_write_strength,
    extra_log_decay,
    head_norm_gain,
    mixer_output_weight,
    expert_input_rows,
    expert_norm_gain,
    routes,
    expert_route_weight,
    gate_weight,
    up_weight,
    down_weight,
):
    EP, T = lax.axis_size("ep"), lax.axis_size("tp")
    Z = T // CORES
    H = head_decay_speed.shape[0]
    width = H * HEAD
    block, model = mixer_input_rows.shape
    toks = expert_input_rows.shape[0]
    half = model // 2
    hidden = gate_weight.shape[2]
    assert block == BLOCK and toks == 8

    vmem = pl.BlockSpec(memory_space=pltpu.VMEM)
    anywhere = pl.BlockSpec(memory_space=pl.ANY)
    dma = pltpu.SemaphoreType.DMA
    V = pltpu.VMEM
    outs = [
        jax.ShapeDtypeStruct((block, model), bf16),
        jax.ShapeDtypeStruct((toks, model), bf16),
    ]
    results = pl.pallas_call(
        functools.partial(fused_kernel, (EP, Z, H)),
        in_specs=[vmem] * 12 + [anywhere] * 7,
        out_specs=[vmem, vmem],
        out_shape=outs,
        scratch_shapes=[
            V((2 * write_strength_projection.shape[1], model), bf16),
            V((model, width), bf16),
            V((model, width), bf16),
            V((model, width), bf16),
            V((model, hidden), bf16),
            V((model, hidden), bf16),
            V((hidden, model), bf16),
            V((Z, CORES, BLOCK, model), bf16),
            V((Z, CORES, width, model), bf16),
            V((EP, CORES, Z, 16, half + HEAD), bf16),
            V((CORES, EP, Z, 16, half), bf16),
            V((EP, Z, 16, half), bf16),
            V((EP, Z, 16, half), bf16),
            V((EP, Z, 16, half), bf16),
            V((Z, 16, half), bf16),
            V((Z, 16, half), bf16),
            V((Z, CORES * BLOCK, width), f32),
            V((Z, CORES * BLOCK, width), bf16),
            V((Z, H, HEAD, 2 * HEAD), f32),
            V((Z, H, HEAD, 2 * HEAD), bf16),
            V((H, HEAD, 2 * HEAD), f32),
            V((2, H, HEAD, HEAD), bf16),
            V((EP, 2, H, HEAD, HEAD), bf16),
            V((H, HEAD, HEAD), f32),
            V((BLOCK, model), f32),
            V((T, BLOCK, width), bf16),
            V((BLOCK, T * width), bf16),
            dma((8,)),
            *[dma((2, Z)), dma((Z,)), dma((Z,)), dma((Z,))],
            *[dma((2, Z)), dma((Z,)), dma((Z, EP)), dma((Z, EP))],
            *[dma((Z, 2)), dma((Z, 2)), dma((Z, EP)), dma((Z, EP))],
            *[dma((Z,)), dma((Z,)), dma((EP,)), dma((EP,)), dma((EP,)), dma((EP,))],
            *[dma((EP, 2)), dma((EP, 2))],
            *[dma((1,)), dma((1,)), dma((EP,)), dma((EP,)), dma((Z,)), dma((Z,))],
            *[dma((T,)), dma((T,))],
        ],
        compiler_params=pltpu.CompilerParams(
            collective_id=0, has_side_effects=True, vmem_limit_bytes=63 * 1024 * 1024
        ),
    )(
        mixer_input_rows,
        mixer_norm_gain.reshape(1, model),
        write_strength_projection.T,
        decay_projection.T,
        largest_write_strength.reshape(1, H),
        head_decay_speed.reshape(1, H),
        extra_log_decay.T,
        head_norm_gain.reshape(1, HEAD),
        expert_input_rows,
        expert_norm_gain.reshape(1, model),
        routes.T,
        expert_route_weight.T,
        query_weight,
        key_weight,
        value_weight,
        mixer_output_weight,
        gate_weight,
        up_weight,
        down_weight,
    )
    return pl.pallas_call(
        hand_over, in_specs=[vmem, vmem], out_specs=[vmem, vmem], out_shape=outs
    )(*results)


def hand_over(mix_in, exp_in, mix_out, exp_out):
    mix_out[...] = mix_in[...]
    exp_out[...] = exp_in[...]


def solution(mesh):
    placed = (
        P(("ep", "tp"), None),
        P(),
        P(None, "tp"),
        P(None, "tp"),
        P(None, "tp"),
        P(),
        P(),
        P("tp"),
        P("tp"),
        P("ep", "tp"),
        P(),
        P("tp", None),
        P(("ep", "tp"), None),
        P(),
        P(("ep", "tp"), None),
        P(("ep", "tp"), None),
        P("ep", None, "tp"),
        P("ep", None, "tp"),
        P("ep", "tp", None),
    )
    return jax.shard_map(
        body,
        mesh=mesh,
        in_specs=placed,
        out_specs=(P(("ep", "tp"), None), P(("ep", "tp"), None)),
        check_vma=False,
    )
```

```python
import functools

import jax
import jax.numpy as jnp
from jax import lax
from jax.experimental import pallas as pl
from jax.experimental.pallas import tpu as pltpu
from jax.sharding import PartitionSpec as P

HEAD = 128
BLOCK = 128
CORES = 2

norm_eps = 1e-06
highest = lax.Precision.HIGHEST
f32 = jnp.float32
bf16 = jnp.bfloat16


def narrow(x):
    return x.astype(bf16)


def halves(x):
    top = narrow(x)
    return top, narrow(x - top.astype(f32))


def mm(a, b):
    return jnp.dot(a, b, preferred_element_type=f32)


def mm_nt(a, b):
    return lax.dot_general(a, b, (((1,), (1,)), ((), ())), preferred_element_type=f32)


def square_full(a, b):
    a_top, a_low = halves(a)
    b_top, b_low = halves(b)
    wide = jnp.concatenate([b_top, b_low], axis=1)
    both = mm(
        jnp.concatenate([a_top, a_low], axis=1), jnp.concatenate([wide, wide], axis=0)
    )
    return both[:, : b.shape[1]] + both[:, b.shape[1] :]


def wide_full(a, b):
    a_top, a_low = halves(a)
    b_top, b_low = halves(b)
    return mm(
        jnp.concatenate([a_top, a_low], axis=1), jnp.concatenate([b_top, b_top], axis=0)
    ) + mm(a_top, b_low)


def silu(x):
    return x / (1.0 + jnp.exp(-x))


def rms_rows(rows, gain):
    wide = rows.astype(f32)
    return wide * lax.rsqrt(jnp.mean(wide * wide, axis=-1, keepdims=True) + norm_eps) * gain


SMALL = 12


def loading_kernel(sizes, *refs):
    raw, rest = refs[:SMALL], refs[SMALL:]
    placed, tiles, sem, others = rest[:9], rest[9 : 9 + SMALL], rest[9 + SMALL], rest[10 + SMALL :]

    def load():
        copies = [
            pltpu.make_async_copy(src, dst, sem.at[i])
            for i, (src, dst) in enumerate(zip(raw, tiles))
        ]
        for copy in copies:
            copy.start()
        return copies

    fused_kernel(sizes, load, *tiles, *placed, *others)


def fused_kernel(
    sizes,
    load_small,
    x_ref,
    xgain_ref,
    wst_ref,
    wdt_ref,
    largest_ref,
    speed_ref,
    extra_ref,
    hgain_ref,
    tok_ref,
    tgain_ref,
    routes_ref,
    weigh_ref,
    wq_hbm,
    wk_hbm,
    wv_hbm,
    wo_hbm,
    wg_hbm,
    wu_hbm,
    wd_hbm,
    mix_ref,
    exp_ref,
    wsmall_ref,
    wq_ref,
    wk_ref,
    wv_ref,
    wg_ref,
    wu_ref,
    wd_ref,
    rows_all,
    wo_all,
    tok_all,
    part_all,
    part_sib,
    part_sum,
    part_in,
    line_all,
    line_in,
    own_all,
    query_all,
    pair_all,
    prefix_all,
    run_ref,
    span_out,
    span_in,
    memory_ref,
    total_ref,
    mixed_all,
    mixed_in,
    local_sem,
    r_s,
    r_r,
    rs_s,
    rs_r,
    w_s,
    w_r,
    wx_s,
    wx_r,
    wh_s,
    wh_r,
    ws_s,
    ws_r,
    t_s,
    t_r,
    te_s,
    te_r,
    ts_s,
    ts_r,
    st_s,
    st_r,
    ps_s,
    ps_r,
    p_s,
    p_r,
    l_s,
    l_r,
    a_s,
    a_r,
):
    EP, Z, H = sizes
    T = Z * CORES
    e = lax.axis_index("ep")
    t = lax.axis_index("tp")
    z = t // CORES
    c = t % CORES
    width = H * HEAD
    model = x_ref.shape[1]
    piece = model // EP
    half = model // 2
    hp = 4 * -(-H // 4)
    relayed = EP == 4

    def remote(src, dst, s, r, **where):
        return pltpu.make_async_remote_copy(
            src_ref=src,
            dst_ref=dst,
            send_sem=s,
            recv_sem=r,
            device_id=where,
            device_id_type=pl.DeviceIdType.MESH,
        )

    def start(copy):
        copy.start()

    def done_send(copy):
        copy.wait_send()

    def done_recv(copy):
        copy.wait_recv()

    def row_copy(zz, step):
        slot = rows_all.at[zz, c]
        d = 0 if step > 0 else 1
        return remote(slot, slot, r_s.at[d, zz], r_r.at[zz], tp=t + step * CORES)

    def row_sibling(zz, core):
        slot = rows_all.at[zz, core]
        return remote(slot, slot, rs_s.at[zz], rs_r.at[zz], tp=z * CORES + 1 - c)

    def wo_slot(zz, core, ee, i):
        rows = width // 2
        return wo_all.at[
            zz, core, i * rows : (i + 1) * rows, pl.ds(pl.multiple_of(ee * piece, piece), piece)
        ]

    def wo_copy(zz, step, i):
        slot = wo_slot(zz, c, e, i)
        d = 0 if step > 0 else 1
        return remote(slot, slot, w_s.at[d, zz, i], w_r.at[zz, i], tp=t + step * CORES)

    def wo_peer(zz, frm, to, i):
        slot = wo_slot(zz, c, frm, i)
        return remote(slot, slot, wx_s.at[zz, to, i], wx_r.at[zz, frm, i], ep=to)

    def wo_half(zz, ee, i):
        slot = wo_slot(zz, c, ee, i)
        return remote(slot, slot, wh_s.at[zz, i], wh_r.at[zz, i], ep=e ^ (2 - i))

    def wo_sibling(zz, core, ee, i):
        slot = wo_slot(zz, core, ee, i)
        return remote(slot, slot, ws_s.at[zz, ee, i], ws_r.at[zz, ee, i], tp=z * CORES + 1 - c)

    def wo_siblings(zz, core, act):
        for ee in range(EP):
            for i in range(2):
                act(wo_sibling(zz, core, ee, i))

    def tok_copy(frm, to):
        slot = tok_all.at[e, c, frm]
        return remote(slot, slot, t_s.at[to], t_r.at[frm], tp=to * CORES + c)

    def tok_peer(frm, to):
        slot = tok_all.at[frm, c]
        return remote(slot, slot, te_s.at[to], te_r.at[frm], ep=to)

    def tok_sibling(ee, core):
        slot = tok_all.at[ee, core]
        return remote(slot, slot, ts_s.at[ee], ts_r.at[ee], tp=z * CORES + 1 - c)

    def state_copy(frm, to, i):
        return remote(
            span_out.at[i], span_in.at[frm, i], st_s.at[to, i], st_r.at[frm, i], ep=to
        )

    def part_sibling():
        return remote(
            part_all.at[1 - c], part_sib, ps_s.at[0], ps_r.at[0], tp=z * CORES + 1 - c
        )

    def part_copy(frm, to):
        return remote(part_sum.at[to], part_in.at[frm], p_s.at[to], p_r.at[frm], ep=to)

    def line_copy(frm, to):
        return remote(
            line_all.at[to], line_in.at[frm], l_s.at[to], l_r.at[frm], tp=to * CORES + c
        )

    def mixed_slot(frm):
        return mixed_in.at[:, pl.ds(pl.multiple_of(frm * width, HEAD), width)]

    def mixed_copy(frm, to):
        return remote(mixed_all.at[to], mixed_slot(frm), a_s.at[to], a_r.at[frm], tp=to)

    def eps(other, act):
        for ee in range(EP):
            pl.when(other(ee))(functools.partial(act, ee))

    def tps(act):
        for tt in range(T):
            pl.when(t != tt)(functools.partial(act, tt))

    def zs(act):
        for zz in range(Z):
            pl.when(z != zz)(functools.partial(act, zz))

    others = lambda ee: e != ee
    peers = (lambda ee: (e ^ 1 == ee) | (e ^ 2 == ee)) if relayed else others

    loads = [
        pltpu.make_async_copy(src, dst, local_sem.at[i])
        for i, (src, dst) in enumerate(
            [
                (wq_hbm, wq_ref),
                (wk_hbm, wk_ref),
                (wv_hbm, wv_ref),
                (wo_hbm, wo_all.at[z, c]),
                (wg_hbm.at[0], wg_ref),
                (wu_hbm.at[0], wu_ref),
                (wd_hbm.at[0], wd_ref),
            ]
        )
    ]

    barrier = pltpu.get_barrier_semaphore()

    def greet_tp(tt):
        pl.semaphore_signal(barrier, inc=1, device_id={"tp": tt}, device_id_type=pl.DeviceIdType.MESH)

    def greet_ep(ee):
        pl.semaphore_signal(barrier, inc=1, device_id={"ep": ee}, device_id_type=pl.DeviceIdType.MESH)

    tps(greet_tp)
    eps(others, greet_ep)
    small = load_small()
    for load in loads[:4]:
        load.start()
    for load in small:
        load.wait()

    rows_all[z, c] = narrow(rms_rows(x_ref[...], xgain_ref[...]))
    wsmall_ref[...] = jnp.concatenate([wst_ref[...], wdt_ref[...]], axis=0)
    tokens = rms_rows(tok_ref[...], tgain_ref[...])
    count = tokens.shape[0]
    diagonal = lax.broadcasted_iota(jnp.int32, (count, count), 0) == lax.broadcasted_iota(
        jnp.int32, (count, count), 1
    )
    lanes = lax.broadcasted_iota(jnp.int32, (count, HEAD), 1)
    share = jnp.zeros((count, HEAD), f32)
    for j in range(routes_ref.shape[0]):

        def column(ref):
            line = ref[j : j + 1, :].astype(f32)
            return jnp.sum(jnp.where(diagonal, line, 0.0), axis=1, keepdims=True)

        share = share + jnp.where(lanes.astype(f32) == column(routes_ref), column(weigh_ref), 0.0)
    share_top = narrow(share).astype(f32)
    tok_all[e, c, z] = narrow(
        jnp.concatenate(
            [
                jnp.concatenate([tokens[:, :half], share_top], axis=1),
                jnp.concatenate([tokens[:, half:], share - share_top], axis=1),
            ],
            axis=0,
        )
    )
    pl.semaphore_wait(barrier, T - 1 + EP - 1)

    zs(lambda zz: start(tok_copy(z, zz)))

    def row_forward(zz):
        pl.when((zz <= z) & (z + 1 < Z))(lambda: start(row_copy(zz, 1)))
        pl.when((zz >= z) & (z >= 1))(lambda: start(row_copy(zz, -1)))
        start(row_sibling(zz, c))

    def row_arrive(zz):
        done_recv(row_copy(zz, 1))
        row_forward(zz)

    end = (z == 0) | (z == Z - 1)
    early_left, early_right = end | (z < Z // 2), end | (z >= Z // 2)

    def wo_out(early):
        for i in range(2):
            pl.when((z + 1 < Z) & (early_right == early))(lambda: start(wo_copy(z, 1, i)))
            pl.when((z >= 1) & (early_left == early))(lambda: start(wo_copy(z, -1, i)))

    def sides(early, s, act):
        pl.when((z - s >= 0) & (early_left == early))(lambda: act(z - s))
        pl.when((z + s < Z) & (early_right == early))(lambda: act(z + s))


    def wo_arrive(zz, which=(0, 1)):
        for i in which:
            done_recv(wo_copy(zz, 1, i))
            pl.when((zz < z) & (z + 1 < Z))(lambda: start(wo_copy(zz, 1, i)))
            pl.when((zz > z) & (z >= 1))(lambda: start(wo_copy(zz, -1, i)))
            if relayed:
                start(wo_peer(zz, e, e ^ (1 + i), i))
                start(wo_peer(zz, e, e ^ (2 - i), i))
            else:
                eps(others, lambda ee: start(wo_peer(zz, e, ee, i)))
            start(wo_sibling(zz, c, e, i))

    def wo_relay(zz):
        if relayed:
            for i in range(2):
                done_recv(wo_peer(zz, e ^ (1 + i), e, i))
                start(wo_half(zz, e ^ (1 + i), i))
                start(wo_sibling(zz, c, e ^ (1 + i), i))

    def wo_collect(zz):
        if relayed:
            for i in range(2):
                done_recv(wo_peer(zz, e ^ (1 + i), e, 1 - i))
                start(wo_sibling(zz, c, e ^ (1 + i), 1 - i))
            for i in range(2):
                done_recv(wo_half(zz, e ^ 3, i))
                start(wo_sibling(zz, c, e ^ 3, i))
        else:

            def pass_on(ee):
                for i in range(2):
                    done_recv(wo_peer(zz, ee, ee, i))
                    start(wo_sibling(zz, c, ee, i))

            eps(others, pass_on)

    def both_sides(s, act):
        pl.when(z - s >= 0)(lambda: act(z - s))
        pl.when(z + s < Z)(lambda: act(z + s))

    row_forward(z)
    loads[3].wait()
    wo_out(True)
    wo_siblings(z, c, start)
    for load in loads[4:]:
        load.start()
    for load in loads[:3]:
        load.wait()

    row = lax.broadcasted_iota(jnp.int32, (BLOCK, BLOCK), 0)
    col = lax.broadcasted_iota(jnp.int32, (BLOCK, BLOCK), 1)

    first_left = max(1, Z - 2)
    midway = Z >= 3

    def process(zz, s):
        causal = row >= col
        strict = row > col
        eye = (row == col).astype(f32)
        upper = (row <= col).astype(f32)
        rows = rows_all[zz].reshape(CORES * BLOCK, model)
        q_all = silu(mm(rows, wq_ref[...]))
        k_all = silu(mm(rows, wk_ref[...]))
        v_all = silu(mm(rows, wv_ref[...]))
        at_rows = pl.ds(pl.multiple_of(zz * CORES * BLOCK, CORES * BLOCK), CORES * BLOCK)
        heads = wst_ref.shape[0]
        every = mm_nt(wsmall_ref[...], rows)
        head = lax.broadcasted_iota(jnp.int32, (2 * heads, CORES * BLOCK), 0)
        place = lax.broadcasted_iota(jnp.int32, (2 * hp, CORES * BLOCK), 0)

        def pick(first):
            return [
                jnp.sum(jnp.where(head == first + t * H + h, every, 0.0), axis=0, keepdims=True)
                for h in range(H)
            ]

        def tiled(lines, first):
            out = jnp.zeros((2 * hp, CORES * BLOCK), f32)
            for h, line in enumerate(lines):
                out = jnp.where(place == first + h, line, out)
            return out

        strength_rows = tiled(
            [
                largest_ref[:, h : h + 1] / (1.0 + jnp.exp(-v))
                for h, v in enumerate(pick(0))
            ],
            0,
        )
        decay_rows = tiled(
            [
                extra_ref[h : h + 1, at_rows]
                - speed_ref[:, h : h + 1]
                * (jnp.maximum(v, 0.0) + jnp.log1p(jnp.exp(-jnp.abs(v))))
                for h, v in enumerate(pick(heads))
            ],
            hp,
        )
        chains = []
        for b in range(CORES):
            at = slice(b * BLOCK, (b + 1) * BLOCK)
            across = jnp.dot(
                decay_rows[:, at], upper, preferred_element_type=f32, precision=highest
            )
            cumulative = across.T
            betas = strength_rows[:, at].T
            for h in range(H):
                of = slice(h * HEAD, (h + 1) * HEAD)
                g = hp + h
                cc = cumulative[:, g : g + 1]
                k = k_all[at, of]
                k = k * lax.rsqrt(jnp.sum(k * k, axis=1, keepdims=True) + 1e-06)
                decays = jnp.exp(jnp.where(causal, cc - across[g : g + 1, :], -1e30))
                chains.append(
                    dict(
                        b=b,
                        h=h,
                        q=q_all[at, of],
                        k=k,
                        v=v_all[at, of],
                        beta=betas[:, h : h + 1],
                        c=cc,
                        decays=decays,
                        last=cumulative[BLOCK - 1 : BLOCK, g : g + 1],
                    )
                )
        for m in chains:
            m["kt"] = m["k"].T
        for m in chains:
            inner = square_full(m["k"], m["kt"])
            m["low"] = jnp.where(strict, inner * m["decays"] * m["beta"], 0.0)
            m["scores"] = narrow(mm(narrow(m["q"]), narrow(m["kt"])) * m["decays"])
        pair_mask = strict & (row // 2 == col // 2)
        for m in chains:
            m["inv"] = eye - jnp.where(pair_mask, m["low"], 0.0)
        if midway:

            @pl.when(s == Z - 1)
            def _():
                both_sides(first_left, lambda other: wo_arrive(other, (0,)))

        size = 2
        while size < BLOCK:
            mask = (row // (2 * size) == col // (2 * size)) & (row // size > col // size)
            for m in chains:
                m["tmp"] = square_full(jnp.where(mask, m["low"], 0.0), m["inv"])
            for m in chains:
                m["inv"] = m["inv"] - square_full(m["inv"], m["tmp"])
            size *= 2
        for m in chains:
            grown = jnp.exp(m["c"])
            m["grown"] = grown
            right = jnp.concatenate(
                [m["v"] * m["beta"], m["k"] * (m["beta"] * grown)], axis=1
            )
            m["solved"] = wide_full(m["inv"], right)
        for m in chains:
            keys_dec_t = (m["k"] * jnp.exp(m["last"] - m["c"])).T
            moved = wide_full(keys_dec_t, m["solved"])
            m["shift"] = moved[:, :HEAD]
            m["map"] = eye * jnp.exp(m["last"]) - moved[:, HEAD:]
            read = mm(m["scores"], narrow(m["solved"]))
            m["own"] = read[:, :HEAD]
            m["query"] = m["q"] * m["grown"] - read[:, HEAD:]
        state = [None] * H
        for m in chains:
            b, h = m["b"], m["h"]
            at, of = slice(b * BLOCK, (b + 1) * BLOCK), slice(h * HEAD, (h + 1) * HEAD)
            if state[h] is None:
                own_all[zz, at, of] = m["own"]
                query_all[zz, at, of] = narrow(m["query"])
                state[h] = jnp.concatenate([m["shift"], m["map"]], axis=1)
            else:
                out = mm(narrow(m["query"]), narrow(state[h]))
                own_all[zz, at, of] = out[:, :HEAD] + m["own"]
                query_all[zz, at, of] = narrow(out[:, HEAD:])
                later = wide_full(m["map"], state[h])
                state[h] = jnp.concatenate(
                    [later[:, :HEAD] + m["shift"], later[:, HEAD:]], axis=1
                )
        for h in range(H):
            pair_all[zz, h] = state[h]

    lines = max(1, min(EP, (2 * BLOCK) // (8 * T)))

    def experts():
        for load in loads[4:]:
            load.wait()
        eps(lambda ee: e >= 0, lambda ee: done_recv(tok_sibling(ee, 1 - c)))
        lane = lax.broadcasted_iota(jnp.int32, (lines * T, 16, HEAD), 2)

        def chunk(i, _):
            span = pl.ds(i * lines, lines)
            got = tok_all[span].reshape(lines * T, 16, half + HEAD).astype(f32)
            count = lines * T * 8
            rows = narrow(
                jnp.concatenate(
                    [
                        got[:, :8, :half].reshape(count, half),
                        got[:, 8:, :half].reshape(count, half),
                    ],
                    axis=1,
                )
            )
            weigh = jnp.sum(
                jnp.where(lane == e, got[:, :, half:], 0.0), axis=2, keepdims=True
            )
            weigh = (weigh[:, :8] + weigh[:, 8:]).reshape(count, 1)
            hidden = narrow(silu(mm(rows, wg_ref[...])) * mm(rows, wu_ref[...]))
            partial = (mm(hidden, wd_ref[...]) * weigh).reshape(lines * T, 8, model)
            both = narrow(
                jnp.concatenate([partial[:, :, :half], partial[:, :, half:]], axis=1)
            ).reshape(lines, CORES, Z, 16, half)
            for core in range(CORES):
                part_all[core, span] = both[:, core]
            return 0

        lax.fori_loop(0, EP // lines, chunk, 0)

    mid, late = min(1, Z - 1), min(2, Z - 1)

    def step(s, _):
        @pl.when(s >= 1)
        def _():
            both_sides(s, row_arrive)

        @pl.when(s == mid)
        def _():
            wo_out(False)
            eps(others, lambda ee: done_recv(tok_peer(ee, ee)))
            eps(lambda ee: e >= 0, lambda ee: start(tok_sibling(ee, c)))

        @pl.when(s == late)
        def _():
            done_recv(part_sibling())
            part_sum[...] = narrow(part_all[c].astype(f32) + part_sib[...].astype(f32))
            eps(others, lambda ee: start(part_copy(e, ee)))

        def side(d, _):
            zz = jnp.where(d == 0, z - s, z + s)

            @pl.when((zz >= 0) & (zz < Z) & ((s > 0) | (d == 0)))
            def _():
                done_recv(row_sibling(zz, 1 - c))
                process(zz, s)

            return 0

        lax.fori_loop(0, 2, side, 0)

        @pl.when(s == 0)
        def _():
            zs(lambda zz: done_recv(tok_copy(zz, zz)))
            eps(others, lambda ee: start(tok_peer(e, ee)))

        @pl.when((s >= 1) & (s <= Z - 3))
        def _():
            sides(True, s, wo_arrive)

        @pl.when(s == mid)
        def _():
            experts()
            start(part_sibling())

        @pl.when((s >= 2) & (s <= Z - 2))
        def _():
            sides(False, s - 1, wo_arrive)
            sides(True, s - 1, wo_relay)

        return 0

    lax.fori_loop(0, Z, step, 0)

    for h in range(H):
        run_ref[h] = pair_all[0, h]

    def compose(zz, _):
        for h in range(H):
            now = run_ref[h]
            prefix_all[zz, h] = narrow(now)
            mine = pair_all[zz, h]
            later = wide_full(mine[:, HEAD:], now)
            run_ref[h] = jnp.concatenate(
                [later[:, :HEAD] + mine[:, :HEAD], later[:, HEAD:]], axis=1
            )
        return 0

    lax.fori_loop(1, Z, compose, 0)
    for h in range(H):
        span_out[0, h] = narrow(run_ref[h, :, :HEAD])
        span_out[1, h] = narrow(run_ref[h, :, HEAD:])
    for ee in reversed(range(EP)):
        pl.when(e < ee)(lambda: start(state_copy(e, ee, 0)))
        pl.when((e < ee) & (e > 0))(lambda: start(state_copy(e, ee, 1)))
    if midway:
        pl.when(end)(lambda: both_sides(first_left, lambda zz: wo_arrive(zz, (1,))))
        pl.when(~end)(lambda: both_sides(first_left, wo_arrive))
    elif Z >= 2:
        both_sides(first_left, wo_arrive)

    def extend(zz, _):
        for h in range(H):
            of = slice(h * HEAD, (h + 1) * HEAD)
            out = mm(query_all[zz, :, of], prefix_all[zz, h])
            own_all[zz, :, of] += out[:, :HEAD]
            query_all[zz, :, of] = narrow(out[:, HEAD:])
        return 0

    lax.fori_loop(1, Z, extend, 0)

    memory_ref[...] = jnp.zeros_like(memory_ref)

    def enter(ee):
        done_recv(state_copy(ee, ee, 0))
        if ee == 0:
            memory_ref[...] = span_in[0, 0].astype(f32)
            return
        done_recv(state_copy(ee, ee, 1))
        for h in range(H):
            top, low = halves(memory_ref[h])
            span_map = span_in[ee, 1, h]
            memory_ref[h] = (
                span_in[ee, 0, h].astype(f32) + mm(span_map, top) + mm(span_map, low)
            )

    for ee in range(EP - 1):
        pl.when(ee < e)(functools.partial(enter, ee))

    def put_off(tt):
        return ((tt // CORES) % (Z - 1) == 0) & (z % (Z - 1) != 0) if Z > 2 else t < 0

    def send_heads(zz):
        for b in range(CORES):
            tt = zz * CORES + b
            pl.when((tt != t) & ~put_off(tt))(lambda: start(mixed_copy(t, tt)))

    def turn(i):
        return lax.rem(z + Z // 2 + i, Z)

    def finish(i, _):
        zz = turn(i)
        for h in range(H):
            of = slice(h * HEAD, (h + 1) * HEAD)
            top, low = halves(memory_ref[h])
            both = mm(query_all[zz, :, of], jnp.concatenate([top, low], axis=1))
            heads = own_all[zz, :, of] + both[:, :HEAD] + both[:, HEAD:]
            scale = lax.rsqrt(jnp.mean(heads * heads, axis=1, keepdims=True) + norm_eps)
            done = narrow(heads * scale * hgain_ref[...])
            for b in range(CORES):
                mixed_all[zz * CORES + b, :, of] = done[b * BLOCK : (b + 1) * BLOCK]
        pl.when(i > 0)(lambda: send_heads(turn(i - 1)))
        return 0

    lax.fori_loop(0, Z, finish, 0)
    send_heads(turn(Z - 1))
    mine = pltpu.make_async_copy(mixed_all.at[t], mixed_slot(t), local_sem.at[7])
    mine.start()
    for s in range(first_left + 1, Z):
        both_sides(s, wo_arrive)
    for s in range(1, first_left):
        sides(False, s, wo_relay)
    if Z >= 2:
        both_sides(first_left, wo_relay)

    eps(others, lambda ee: done_recv(part_copy(ee, ee)))
    part_in[e] = part_sum[e]
    total = part_in[0].astype(f32)
    for ee in range(1, EP):
        total = total + part_in[ee].astype(f32)
    line_all[...] = narrow(total)
    line_in[z] = line_all[z]
    zs(lambda zz: start(line_copy(z, zz)))

    def project(zz):
        for b in range(CORES):
            tt = zz * CORES + b
            pl.when(tt != t)(lambda: done_recv(mixed_copy(tt, tt)))
        wo_siblings(zz, 1 - c, done_recv)
        heads = mixed_in[:, pl.ds(pl.multiple_of(zz * CORES * width, HEAD), CORES * width)]
        total_ref[...] += mm(heads, wo_all[zz].reshape(CORES * width, model))

    total_ref[...] = jnp.zeros_like(total_ref)
    tps(lambda tt: pl.when(put_off(tt))(lambda: start(mixed_copy(t, tt))))
    for s in range(first_left + 1, Z):
        both_sides(s, wo_relay)
    for s in range(1, first_left + 1):
        both_sides(s, wo_collect)
    mine.wait()

    def near(s, _):
        def side(d, _):
            zz = jnp.where(d == 0, z - s, z + s)

            @pl.when((zz >= 0) & (zz < Z) & ((s > 0) | (d == 0)))
            def _():
                @pl.when((s > first_left))
                def _():
                    wo_collect(zz)

                project(zz)

            return 0

        lax.fori_loop(0, 2, side, 0)
        return 0

    lax.fori_loop(0, Z, near, 0)
    mix_ref[...] = narrow(total_ref[...])

    zs(lambda zz: done_recv(line_copy(zz, zz)))
    result = line_in[0].astype(f32)
    for zz in range(1, Z):
        result = result + line_in[zz].astype(f32)
    exp_ref[...] = narrow(jnp.concatenate([result[:8], result[8:]], axis=1))

    zs(lambda zz: done_send(tok_copy(z, zz)))

    def drain(zz, _):
        for right in (lambda step: row_copy(zz, step), lambda step: wo_copy(zz, step, 0), lambda step: wo_copy(zz, step, 1)):
            pl.when((zz <= z) & (z + 1 < Z))(lambda: done_send(right(1)))
            pl.when((zz >= z) & (z >= 1))(lambda: done_send(right(-1)))
        done_send(row_sibling(zz, c))
        wo_siblings(zz, c, done_send)

        @pl.when(zz != z)
        def _():
            for i in range(2):
                eps(peers, lambda ee: done_send(wo_peer(zz, e, ee, i)))
            if relayed:
                for i in range(2):
                    done_send(wo_half(zz, e ^ (1 + i), i))

        return 0

    lax.fori_loop(0, Z, drain, 0)
    eps(others, lambda ee: done_send(tok_peer(e, ee)))
    eps(lambda ee: e >= 0, lambda ee: done_send(tok_sibling(ee, c)))
    eps(lambda ee: e < ee, lambda ee: done_send(state_copy(e, ee, 0)))
    eps(lambda ee: (e < ee) & (e > 0), lambda ee: done_send(state_copy(e, ee, 1)))
    eps(others, lambda ee: done_send(part_copy(e, ee)))
    done_send(part_sibling())
    zs(lambda zz: done_send(line_copy(z, zz)))
    tps(lambda tt: done_send(mixed_copy(t, tt)))


def body(
    mixer_input_rows,
    mixer_norm_gain,
    query_weight,
    key_weight,
    value_weight,
    write_strength_projection,
    decay_projection,
    head_decay_speed,
    largest_write_strength,
    extra_log_decay,
    head_norm_gain,
    mixer_output_weight,
    expert_input_rows,
    expert_norm_gain,
    routes,
    expert_route_weight,
    gate_weight,
    up_weight,
    down_weight,
):
    EP, T = lax.axis_size("ep"), lax.axis_size("tp")
    Z = T // CORES
    H = head_decay_speed.shape[0]
    width = H * HEAD
    block, model = mixer_input_rows.shape
    toks = expert_input_rows.shape[0]
    half = model // 2
    hidden = gate_weight.shape[2]
    assert block == BLOCK and toks == 8

    vmem = pl.BlockSpec(memory_space=pltpu.VMEM)
    anywhere = pl.BlockSpec(memory_space=pl.ANY)
    dma = pltpu.SemaphoreType.DMA
    V = pltpu.VMEM
    outs = [
        jax.ShapeDtypeStruct((block, model), bf16),
        jax.ShapeDtypeStruct((toks, model), bf16),
    ]
    small = [
        mixer_input_rows,
        mixer_norm_gain.reshape(1, model),
        write_strength_projection.T,
        decay_projection.T,
        largest_write_strength.reshape(1, H),
        head_decay_speed.reshape(1, H),
        extra_log_decay.T,
        head_norm_gain.reshape(1, HEAD),
        expert_input_rows,
        expert_norm_gain.reshape(1, model),
        routes.T,
        expert_route_weight.T,
    ]
    scratch = [
        *[V(v.shape, v.dtype) for v in small],
        dma((SMALL,)),
        V((2 * write_strength_projection.shape[1], model), bf16),
        V((model, width), bf16),
        V((model, width), bf16),
        V((model, width), bf16),
        V((model, hidden), bf16),
        V((model, hidden), bf16),
        V((hidden, model), bf16),
        V((Z, CORES, BLOCK, model), bf16),
        V((Z, CORES, width, model), bf16),
        V((EP, CORES, Z, 16, half + HEAD), bf16),
        V((CORES, EP, Z, 16, half), bf16),
        V((EP, Z, 16, half), bf16),
        V((EP, Z, 16, half), bf16),
        V((EP, Z, 16, half), bf16),
        V((Z, 16, half), bf16),
        V((Z, 16, half), bf16),
        V((Z, CORES * BLOCK, width), f32),
        V((Z, CORES * BLOCK, width), bf16),
        V((Z, H, HEAD, 2 * HEAD), f32),
        V((Z, H, HEAD, 2 * HEAD), bf16),
        V((H, HEAD, 2 * HEAD), f32),
        V((2, H, HEAD, HEAD), bf16),
        V((EP, 2, H, HEAD, HEAD), bf16),
        V((H, HEAD, HEAD), f32),
        V((BLOCK, model), f32),
        V((T, BLOCK, width), bf16),
        V((BLOCK, T * width), bf16),
        dma((8,)),
        *[dma((2, Z)), dma((Z,)), dma((Z,)), dma((Z,))],
        *[dma((2, Z, 2)), dma((Z, 2)), dma((Z, EP, 2)), dma((Z, EP, 2))],
        *[dma((Z, 2)), dma((Z, 2)), dma((Z, EP, 2)), dma((Z, EP, 2))],
        *[dma((Z,)), dma((Z,)), dma((EP,)), dma((EP,)), dma((EP,)), dma((EP,))],
        *[dma((EP, 2)), dma((EP, 2))],
        *[dma((1,)), dma((1,)), dma((EP,)), dma((EP,)), dma((Z,)), dma((Z,))],
        *[dma((T,)), dma((T,))],
    ]
    results = pl.pallas_call(
        functools.partial(loading_kernel, (EP, Z, H)),
        in_specs=[anywhere] * (SMALL + 7),
        out_specs=[vmem, vmem],
        out_shape=outs,
        scratch_shapes=scratch,
        compiler_params=pltpu.CompilerParams(
            collective_id=0, has_side_effects=True, vmem_limit_bytes=63 << 20
        ),
    )(
        *small,
        query_weight,
        key_weight,
        value_weight,
        mixer_output_weight,
        gate_weight,
        up_weight,
        down_weight,
    )
    return pl.pallas_call(
        hand_over,
        in_specs=[vmem, vmem],
        out_specs=[anywhere, anywhere],
        out_shape=outs,
        scratch_shapes=[dma((2,))],
    )(*results)


def hand_over(mix_in, exp_in, mix_out, exp_out, sem):
    copies = [
        pltpu.make_async_copy(mix_in, mix_out, sem.at[0]),
        pltpu.make_async_copy(exp_in, exp_out, sem.at[1]),
    ]
    for copy in copies:
        copy.start()
    for copy in copies:
        copy.wait()


def solution(mesh):
    placed = (
        P(("ep", "tp"), None),
        P(),
        P(None, "tp"),
        P(None, "tp"),
        P(None, "tp"),
        P(),
        P(),
        P("tp"),
        P("tp"),
        P("ep", "tp"),
        P(),
        P("tp", None),
        P(("ep", "tp"), None),
        P(),
        P(("ep", "tp"), None),
        P(("ep", "tp"), None),
        P("ep", None, "tp"),
        P("ep", None, "tp"),
        P("ep", "tp", None),
    )
    return jax.shard_map(
        body,
        mesh=mesh,
        in_specs=placed,
        out_specs=(P(("ep", "tp"), None), P(("ep", "tp"), None)),
        check_vma=False,
    )
```

```python
import functools

import jax
import jax.numpy as jnp
from jax import lax
from jax.experimental import pallas as pl
from jax.experimental.pallas import tpu as pltpu
from jax.sharding import PartitionSpec as P

HEAD = 128
BLOCK = 128
CORES = 2

norm_eps = 1e-06
highest = lax.Precision.HIGHEST
f32 = jnp.float32
bf16 = jnp.bfloat16


def narrow(x):
    return x.astype(bf16)


def halves(x):
    top = narrow(x)
    return top, narrow(x - top.astype(f32))


def mm(a, b):
    return jnp.dot(a, b, preferred_element_type=f32)


def mm_nt(a, b):
    return lax.dot_general(a, b, (((1,), (1,)), ((), ())), preferred_element_type=f32)


def square_full(a, b):
    a_top, a_low = halves(a)
    b_top, b_low = halves(b)
    wide = jnp.concatenate([b_top, b_low], axis=1)
    both = mm(
        jnp.concatenate([a_top, a_low], axis=1), jnp.concatenate([wide, wide], axis=0)
    )
    return both[:, : b.shape[1]] + both[:, b.shape[1] :]


def wide_full(a, b):
    a_top, a_low = halves(a)
    b_top, b_low = halves(b)
    return mm(
        jnp.concatenate([a_top, a_low], axis=1), jnp.concatenate([b_top, b_top], axis=0)
    ) + mm(a_top, b_low)


def silu(x):
    return x / (1.0 + jnp.exp(-x))


def rms_rows(rows, gain):
    wide = rows.astype(f32)
    return wide * lax.rsqrt(jnp.mean(wide * wide, axis=-1, keepdims=True) + norm_eps) * gain


SMALL = 12


def loading_kernel(sizes, *refs):
    raw, rest = refs[:SMALL], refs[SMALL:]
    placed, tiles, sem, others = rest[:9], rest[9 : 9 + SMALL], rest[9 + SMALL], rest[10 + SMALL :]

    def load():
        copies = [
            pltpu.make_async_copy(src, dst, sem.at[i])
            for i, (src, dst) in enumerate(zip(raw, tiles))
        ]
        for copy in copies:
            copy.start()
        return copies

    fused_kernel(sizes, load, *tiles, *placed, *others)


def fused_kernel(
    sizes,
    load_small,
    x_ref,
    xgain_ref,
    wst_ref,
    wdt_ref,
    largest_ref,
    speed_ref,
    extra_ref,
    hgain_ref,
    tok_ref,
    tgain_ref,
    routes_ref,
    weigh_ref,
    wq_hbm,
    wk_hbm,
    wv_hbm,
    wo_hbm,
    wg_hbm,
    wu_hbm,
    wd_hbm,
    mix_ref,
    exp_ref,
    wsmall_ref,
    wq_ref,
    wk_ref,
    wv_ref,
    wg_ref,
    wu_ref,
    wd_ref,
    rows_all,
    wo_all,
    tok_all,
    part_all,
    part_sib,
    part_sum,
    part_in,
    line_all,
    line_in,
    own_all,
    query_all,
    pair_all,
    prefix_all,
    run_ref,
    span_out,
    span_in,
    memory_ref,
    total_ref,
    mixed_all,
    mixed_in,
    local_sem,
    r_s,
    r_r,
    rs_s,
    rs_r,
    w_s,
    w_r,
    wx_s,
    wx_r,
    wh_s,
    wh_r,
    ws_s,
    ws_r,
    t_s,
    t_r,
    te_s,
    te_r,
    ts_s,
    ts_r,
    st_s,
    st_r,
    ps_s,
    ps_r,
    p_s,
    p_r,
    l_s,
    l_r,
    a_s,
    a_r,
):
    EP, Z, H = sizes
    T = Z * CORES
    e = lax.axis_index("ep")
    t = lax.axis_index("tp")
    z = t // CORES
    c = t % CORES
    width = H * HEAD
    model = x_ref.shape[1]
    piece = model // EP
    half = model // 2
    hp = 4 * -(-H // 4)
    relayed = EP == 4

    def remote(src, dst, s, r, **where):
        return pltpu.make_async_remote_copy(
            src_ref=src,
            dst_ref=dst,
            send_sem=s,
            recv_sem=r,
            device_id=where,
            device_id_type=pl.DeviceIdType.MESH,
        )

    def start(copy):
        copy.start()

    def done_send(copy):
        copy.wait_send()

    def done_recv(copy):
        copy.wait_recv()

    def row_copy(zz, step):
        slot = rows_all.at[zz, c]
        d = 0 if step > 0 else 1
        return remote(slot, slot, r_s.at[d, zz], r_r.at[zz], tp=t + step * CORES)

    def row_sibling(zz, core):
        slot = rows_all.at[zz, core]
        return remote(slot, slot, rs_s.at[zz], rs_r.at[zz], tp=z * CORES + 1 - c)

    def wo_slot(zz, core, ee, i):
        rows = width // 2
        return wo_all.at[
            zz, core, i * rows : (i + 1) * rows, pl.ds(pl.multiple_of(ee * piece, piece), piece)
        ]

    def wo_copy(zz, step, i):
        slot = wo_slot(zz, c, e, i)
        d = 0 if step > 0 else 1
        return remote(slot, slot, w_s.at[d, zz, i], w_r.at[zz, i], tp=t + step * CORES)

    def wo_peer(zz, frm, to, i):
        slot = wo_slot(zz, c, frm, i)
        return remote(slot, slot, wx_s.at[zz, to, i], wx_r.at[zz, frm, i], ep=to)

    def wo_half(zz, ee, i):
        slot = wo_slot(zz, c, ee, i)
        return remote(slot, slot, wh_s.at[zz, i], wh_r.at[zz, i], ep=e ^ (2 - i))

    def wo_sibling(zz, core, ee, i):
        slot = wo_slot(zz, core, ee, i)
        return remote(slot, slot, ws_s.at[zz, ee, i], ws_r.at[zz, ee, i], tp=z * CORES + 1 - c)

    def wo_siblings(zz, core, act):
        for ee in range(EP):
            for i in range(2):
                act(wo_sibling(zz, core, ee, i))

    def tok_copy(frm, to):
        slot = tok_all.at[e, c, frm]
        return remote(slot, slot, t_s.at[to], t_r.at[frm], tp=to * CORES + c)

    def tok_peer(frm, to):
        slot = tok_all.at[frm, c]
        return remote(slot, slot, te_s.at[to], te_r.at[frm], ep=to)

    def tok_sibling(ee, core):
        slot = tok_all.at[ee, core]
        return remote(slot, slot, ts_s.at[ee], ts_r.at[ee], tp=z * CORES + 1 - c)

    def state_copy(frm, to, i):
        return remote(
            span_out.at[i], span_in.at[frm, i], st_s.at[to, i], st_r.at[frm, i], ep=to
        )

    def part_sibling():
        return remote(
            part_all.at[1 - c], part_sib, ps_s.at[0], ps_r.at[0], tp=z * CORES + 1 - c
        )

    def part_copy(frm, to):
        return remote(part_sum.at[to], part_in.at[frm], p_s.at[to], p_r.at[frm], ep=to)

    def line_copy(frm, to):
        return remote(
            line_all.at[to], line_in.at[frm], l_s.at[to], l_r.at[frm], tp=to * CORES + c
        )

    def mixed_slot(frm):
        return mixed_in.at[:, pl.ds(pl.multiple_of(frm * width, HEAD), width)]

    def mixed_copy(frm, to):
        return remote(mixed_all.at[to], mixed_slot(frm), a_s.at[to], a_r.at[frm], tp=to)

    def eps(other, act):
        for ee in range(EP):
            pl.when(other(ee))(functools.partial(act, ee))

    def tps(act):
        for tt in range(T):
            pl.when(t != tt)(functools.partial(act, tt))

    def zs(act):
        for zz in range(Z):
            pl.when(z != zz)(functools.partial(act, zz))

    others = lambda ee: e != ee
    peers = (lambda ee: (e ^ 1 == ee) | (e ^ 2 == ee)) if relayed else others

    loads = [
        pltpu.make_async_copy(src, dst, local_sem.at[i])
        for i, (src, dst) in enumerate(
            [
                (wq_hbm, wq_ref),
                (wk_hbm, wk_ref),
                (wv_hbm, wv_ref),
                (wo_hbm, wo_all.at[z, c]),
                (wg_hbm.at[0], wg_ref),
                (wu_hbm.at[0], wu_ref),
                (wd_hbm.at[0], wd_ref),
            ]
        )
    ]

    barrier = pltpu.get_barrier_semaphore()

    def greet_tp(tt):
        pl.semaphore_signal(barrier, inc=1, device_id={"tp": tt}, device_id_type=pl.DeviceIdType.MESH)

    def greet_ep(ee):
        pl.semaphore_signal(barrier, inc=1, device_id={"ep": ee}, device_id_type=pl.DeviceIdType.MESH)

    tps(greet_tp)
    eps(others, greet_ep)
    small = load_small()
    for load in loads[:4]:
        load.start()
    for load in small:
        load.wait()

    rows_all[z, c] = narrow(rms_rows(x_ref[...], xgain_ref[...]))
    wsmall_ref[...] = jnp.concatenate([wst_ref[...], wdt_ref[...]], axis=0)
    tokens = rms_rows(tok_ref[...], tgain_ref[...])
    count = tokens.shape[0]
    diagonal = lax.broadcasted_iota(jnp.int32, (count, count), 0) == lax.broadcasted_iota(
        jnp.int32, (count, count), 1
    )
    lanes = lax.broadcasted_iota(jnp.int32, (count, HEAD), 1)
    share = jnp.zeros((count, HEAD), f32)
    for j in range(routes_ref.shape[0]):

        def column(ref):
            line = ref[j : j + 1, :].astype(f32)
            return jnp.sum(jnp.where(diagonal, line, 0.0), axis=1, keepdims=True)

        share = share + jnp.where(lanes.astype(f32) == column(routes_ref), column(weigh_ref), 0.0)
    share_top = narrow(share).astype(f32)
    tok_all[e, c, z] = narrow(
        jnp.concatenate(
            [
                jnp.concatenate([tokens[:, :half], share_top], axis=1),
                jnp.concatenate([tokens[:, half:], share - share_top], axis=1),
            ],
            axis=0,
        )
    )
    pl.semaphore_wait(barrier, T - 1 + EP - 1)

    zs(lambda zz: start(tok_copy(z, zz)))

    def row_forward(zz):
        pl.when((zz <= z) & (z + 1 < Z))(lambda: start(row_copy(zz, 1)))
        pl.when((zz >= z) & (z >= 1))(lambda: start(row_copy(zz, -1)))
        start(row_sibling(zz, c))

    def row_arrive(zz):
        done_recv(row_copy(zz, 1))
        row_forward(zz)

    end = (z == 0) | (z == Z - 1)
    early_left, early_right = end | (z < Z // 2), end | (z >= Z // 2)

    def wo_out(early):
        for i in range(2):
            pl.when((z + 1 < Z) & (early_right == early))(lambda: start(wo_copy(z, 1, i)))
            pl.when((z >= 1) & (early_left == early))(lambda: start(wo_copy(z, -1, i)))

    def sides(early, s, act):
        pl.when((z - s >= 0) & (early_left == early))(lambda: act(z - s))
        pl.when((z + s < Z) & (early_right == early))(lambda: act(z + s))


    def wo_arrive(zz, which=(0, 1)):
        for i in which:
            done_recv(wo_copy(zz, 1, i))
            pl.when((zz < z) & (z + 1 < Z))(lambda: start(wo_copy(zz, 1, i)))
            pl.when((zz > z) & (z >= 1))(lambda: start(wo_copy(zz, -1, i)))
            if relayed:
                start(wo_peer(zz, e, e ^ (1 + i), i))
                start(wo_peer(zz, e, e ^ (2 - i), i))
            else:
                eps(others, lambda ee: start(wo_peer(zz, e, ee, i)))
            start(wo_sibling(zz, c, e, i))

    def wo_relay(zz):
        if relayed:
            for i in range(2):
                done_recv(wo_peer(zz, e ^ (1 + i), e, i))
                start(wo_half(zz, e ^ (1 + i), i))
                start(wo_sibling(zz, c, e ^ (1 + i), i))

    def wo_collect(zz):
        if relayed:
            for i in range(2):
                done_recv(wo_peer(zz, e ^ (1 + i), e, 1 - i))
                start(wo_sibling(zz, c, e ^ (1 + i), 1 - i))
            for i in range(2):
                done_recv(wo_half(zz, e ^ 3, i))
                start(wo_sibling(zz, c, e ^ 3, i))
        else:

            def pass_on(ee):
                for i in range(2):
                    done_recv(wo_peer(zz, ee, ee, i))
                    start(wo_sibling(zz, c, ee, i))

            eps(others, pass_on)

    def both_sides(s, act):
        pl.when(z - s >= 0)(lambda: act(z - s))
        pl.when(z + s < Z)(lambda: act(z + s))

    row_forward(z)
    loads[3].wait()
    wo_out(True)
    wo_siblings(z, c, start)
    for load in loads[4:]:
        load.start()
    for load in loads[:3]:
        load.wait()

    row = lax.broadcasted_iota(jnp.int32, (BLOCK, BLOCK), 0)
    col = lax.broadcasted_iota(jnp.int32, (BLOCK, BLOCK), 1)

    first_left = max(1, Z - 2)
    midway = Z >= 3

    def process(zz, s):
        causal = row >= col
        strict = row > col
        eye = (row == col).astype(f32)
        upper = (row <= col).astype(f32)
        rows = rows_all[zz].reshape(CORES * BLOCK, model)
        q_all = silu(mm(rows, wq_ref[...]))
        k_all = silu(mm(rows, wk_ref[...]))
        v_all = silu(mm(rows, wv_ref[...]))
        at_rows = pl.ds(pl.multiple_of(zz * CORES * BLOCK, CORES * BLOCK), CORES * BLOCK)
        heads = wst_ref.shape[0]
        every = mm_nt(wsmall_ref[...], rows)
        head = lax.broadcasted_iota(jnp.int32, (2 * heads, CORES * BLOCK), 0)
        place = lax.broadcasted_iota(jnp.int32, (2 * hp, CORES * BLOCK), 0)

        def pick(first):
            return [
                jnp.sum(jnp.where(head == first + t * H + h, every, 0.0), axis=0, keepdims=True)
                for h in range(H)
            ]

        def tiled(lines, first):
            out = jnp.zeros((2 * hp, CORES * BLOCK), f32)
            for h, line in enumerate(lines):
                out = jnp.where(place == first + h, line, out)
            return out

        strength_rows = tiled(
            [
                largest_ref[:, h : h + 1] / (1.0 + jnp.exp(-v))
                for h, v in enumerate(pick(0))
            ],
            0,
        )
        decay_rows = tiled(
            [
                extra_ref[h : h + 1, at_rows]
                - speed_ref[:, h : h + 1]
                * (jnp.maximum(v, 0.0) + jnp.log1p(jnp.exp(-jnp.abs(v))))
                for h, v in enumerate(pick(heads))
            ],
            hp,
        )
        chains = []
        for b in range(CORES):
            at = slice(b * BLOCK, (b + 1) * BLOCK)
            across = jnp.dot(
                decay_rows[:, at], upper, preferred_element_type=f32, precision=highest
            )
            cumulative = across.T
            betas = strength_rows[:, at].T
            for h in range(H):
                of = slice(h * HEAD, (h + 1) * HEAD)
                g = hp + h
                cc = cumulative[:, g : g + 1]
                k = k_all[at, of]
                k = k * lax.rsqrt(jnp.sum(k * k, axis=1, keepdims=True) + 1e-06)
                decays = jnp.exp(jnp.where(causal, cc - across[g : g + 1, :], -1e30))
                chains.append(
                    dict(
                        b=b,
                        h=h,
                        q=q_all[at, of],
                        k=k,
                        v=v_all[at, of],
                        beta=betas[:, h : h + 1],
                        c=cc,
                        decays=decays,
                        last=cumulative[BLOCK - 1 : BLOCK, g : g + 1],
                    )
                )
        for m in chains:
            m["kt"] = m["k"].T
        for m in chains:
            inner = square_full(m["k"], m["kt"])
            m["low"] = jnp.where(strict, inner * m["decays"] * m["beta"], 0.0)
            m["scores"] = narrow(mm(narrow(m["q"]), narrow(m["kt"])) * m["decays"])
        pair_mask = strict & (row // 2 == col // 2)
        for m in chains:
            m["inv"] = eye - jnp.where(pair_mask, m["low"], 0.0)
        if midway:

            @pl.when(s == Z - 1)
            def _():
                both_sides(first_left, lambda other: wo_arrive(other, (0,)))

        size = 2
        while size < BLOCK:
            mask = (row // (2 * size) == col // (2 * size)) & (row // size > col // size)
            for m in chains:
                m["tmp"] = square_full(jnp.where(mask, m["low"], 0.0), m["inv"])
            for m in chains:
                m["inv"] = m["inv"] - square_full(m["inv"], m["tmp"])
            size *= 2
        for m in chains:
            grown = jnp.exp(m["c"])
            m["grown"] = grown
            right = jnp.concatenate(
                [m["v"] * m["beta"], m["k"] * (m["beta"] * grown)], axis=1
            )
            m["solved"] = wide_full(m["inv"], right)
        for m in chains:
            keys_dec_t = (m["k"] * jnp.exp(m["last"] - m["c"])).T
            moved = wide_full(keys_dec_t, m["solved"])
            m["shift"] = moved[:, :HEAD]
            m["map"] = eye * jnp.exp(m["last"]) - moved[:, HEAD:]
            read = mm(m["scores"], narrow(m["solved"]))
            m["own"] = read[:, :HEAD]
            m["query"] = m["q"] * m["grown"] - read[:, HEAD:]
        state = [None] * H
        for m in chains:
            b, h = m["b"], m["h"]
            at, of = slice(b * BLOCK, (b + 1) * BLOCK), slice(h * HEAD, (h + 1) * HEAD)
            if state[h] is None:
                own_all[zz, at, of] = m["own"]
                query_all[zz, at, of] = narrow(m["query"])
                state[h] = jnp.concatenate([m["shift"], m["map"]], axis=1)
            else:
                out = mm(narrow(m["query"]), narrow(state[h]))
                own_all[zz, at, of] = out[:, :HEAD] + m["own"]
                query_all[zz, at, of] = narrow(out[:, HEAD:])
                later = wide_full(m["map"], state[h])
                state[h] = jnp.concatenate(
                    [later[:, :HEAD] + m["shift"], later[:, HEAD:]], axis=1
                )
        for h in range(H):
            pair_all[zz, h] = state[h]

    lines = max(1, min(EP, (2 * BLOCK) // (8 * T)))

    def experts():
        for load in loads[4:]:
            load.wait()
        eps(lambda ee: e >= 0, lambda ee: done_recv(tok_sibling(ee, 1 - c)))
        lane = lax.broadcasted_iota(jnp.int32, (lines * T, 16, HEAD), 2)

        def chunk(i, _):
            span = pl.ds(i * lines, lines)
            got = tok_all[span].reshape(lines * T, 16, half + HEAD).astype(f32)
            count = lines * T * 8
            rows = narrow(
                jnp.concatenate(
                    [
                        got[:, :8, :half].reshape(count, half),
                        got[:, 8:, :half].reshape(count, half),
                    ],
                    axis=1,
                )
            )
            weigh = jnp.sum(
                jnp.where(lane == e, got[:, :, half:], 0.0), axis=2, keepdims=True
            )
            weigh = (weigh[:, :8] + weigh[:, 8:]).reshape(count, 1)
            hidden = narrow(silu(mm(rows, wg_ref[...])) * mm(rows, wu_ref[...]))
            partial = (mm(hidden, wd_ref[...]) * weigh).reshape(lines * T, 8, model)
            both = narrow(
                jnp.concatenate([partial[:, :, :half], partial[:, :, half:]], axis=1)
            ).reshape(lines, CORES, Z, 16, half)
            for core in range(CORES):
                part_all[core, span] = both[:, core]
            return 0

        lax.fori_loop(0, EP // lines, chunk, 0)

    mid, late = min(1, Z - 1), min(2, Z - 1)

    def step(s, _):
        @pl.when(s >= 1)
        def _():
            both_sides(s, row_arrive)

        @pl.when(s == mid)
        def _():
            wo_out(False)
            eps(others, lambda ee: done_recv(tok_peer(ee, ee)))
            eps(lambda ee: e >= 0, lambda ee: start(tok_sibling(ee, c)))

        @pl.when(s == late)
        def _():
            done_recv(part_sibling())
            part_sum[...] = narrow(part_all[c].astype(f32) + part_sib[...].astype(f32))
            eps(others, lambda ee: start(part_copy(e, ee)))

        def side(d, _):
            zz = jnp.where(d == 0, z - s, z + s)

            @pl.when((zz >= 0) & (zz < Z) & ((s > 0) | (d == 0)))
            def _():
                done_recv(row_sibling(zz, 1 - c))
                process(zz, s)

            return 0

        lax.fori_loop(0, 2, side, 0)

        @pl.when(s == 0)
        def _():
            zs(lambda zz: done_recv(tok_copy(zz, zz)))
            eps(others, lambda ee: start(tok_peer(e, ee)))

        @pl.when((s >= 1) & (s <= Z - 3))
        def _():
            sides(True, s, wo_arrive)

        @pl.when(s == mid)
        def _():
            experts()
            start(part_sibling())

        @pl.when((s >= 2) & (s <= Z - 2))
        def _():
            sides(False, s - 1, wo_arrive)
            sides(True, s - 1, wo_relay)

        return 0

    lax.fori_loop(0, Z, step, 0)

    for h in range(H):
        run_ref[h] = pair_all[0, h]

    def compose(zz, _):
        for h in range(H):
            now = run_ref[h]
            prefix_all[zz, h] = narrow(now)
            mine = pair_all[zz, h]
            later = wide_full(mine[:, HEAD:], now)
            run_ref[h] = jnp.concatenate(
                [later[:, :HEAD] + mine[:, :HEAD], later[:, HEAD:]], axis=1
            )
        return 0

    lax.fori_loop(1, Z, compose, 0)
    for h in range(H):
        span_out[0, h] = narrow(run_ref[h, :, :HEAD])
        span_out[1, h] = narrow(run_ref[h, :, HEAD:])
    for ee in reversed(range(EP)):
        pl.when(e < ee)(lambda: start(state_copy(e, ee, 0)))
        pl.when((e < ee) & (e > 0))(lambda: start(state_copy(e, ee, 1)))
    if midway:
        pl.when(end)(lambda: both_sides(first_left, lambda zz: wo_arrive(zz, (1,))))
        pl.when(~end)(lambda: both_sides(first_left, wo_arrive))
    elif Z >= 2:
        both_sides(first_left, wo_arrive)

    def extend(zz, _):
        for h in range(H):
            of = slice(h * HEAD, (h + 1) * HEAD)
            out = mm(query_all[zz, :, of], prefix_all[zz, h])
            own_all[zz, :, of] += out[:, :HEAD]
            query_all[zz, :, of] = narrow(out[:, HEAD:])
        return 0

    lax.fori_loop(1, Z, extend, 0)

    for s in range(first_left + 1, Z):
        both_sides(s, wo_arrive)

    memory_ref[...] = jnp.zeros_like(memory_ref)

    def enter(ee):
        done_recv(state_copy(ee, ee, 0))
        if ee == 0:
            memory_ref[...] = span_in[0, 0].astype(f32)
            return
        done_recv(state_copy(ee, ee, 1))
        for h in range(H):
            top, low = halves(memory_ref[h])
            span_map = span_in[ee, 1, h]
            memory_ref[h] = (
                span_in[ee, 0, h].astype(f32) + mm(span_map, top) + mm(span_map, low)
            )

    for ee in range(EP - 1):
        pl.when(ee < e)(functools.partial(enter, ee))

    def put_off(tt):
        return ((tt // CORES) % (Z - 1) == 0) & (z % (Z - 1) != 0) if Z > 2 else t < 0

    def send_heads(zz):
        for b in range(CORES):
            tt = zz * CORES + b
            pl.when((tt != t) & ~put_off(tt))(lambda: start(mixed_copy(t, tt)))

    def turn(i):
        return lax.rem(z + Z // 2 + i, Z)

    def finish(i, _):
        zz = turn(i)
        for h in range(H):
            of = slice(h * HEAD, (h + 1) * HEAD)
            top, low = halves(memory_ref[h])
            both = mm(query_all[zz, :, of], jnp.concatenate([top, low], axis=1))
            heads = own_all[zz, :, of] + both[:, :HEAD] + both[:, HEAD:]
            scale = lax.rsqrt(jnp.mean(heads * heads, axis=1, keepdims=True) + norm_eps)
            done = narrow(heads * scale * hgain_ref[...])
            for b in range(CORES):
                mixed_all[zz * CORES + b, :, of] = done[b * BLOCK : (b + 1) * BLOCK]
        pl.when(i > 0)(lambda: send_heads(turn(i - 1)))
        return 0

    lax.fori_loop(0, Z, finish, 0)
    send_heads(turn(Z - 1))
    mine = pltpu.make_async_copy(mixed_all.at[t], mixed_slot(t), local_sem.at[7])
    mine.start()
    for s in range(1, first_left):
        sides(False, s, wo_relay)
    if Z >= 2:
        both_sides(first_left, wo_relay)

    eps(others, lambda ee: done_recv(part_copy(ee, ee)))
    part_in[e] = part_sum[e]
    total = part_in[0].astype(f32)
    for ee in range(1, EP):
        total = total + part_in[ee].astype(f32)
    line_all[...] = narrow(total)
    line_in[z] = line_all[z]
    zs(lambda zz: start(line_copy(z, zz)))

    def project(zz):
        for b in range(CORES):
            tt = zz * CORES + b
            pl.when(tt != t)(lambda: done_recv(mixed_copy(tt, tt)))
        wo_siblings(zz, 1 - c, done_recv)
        heads = mixed_in[:, pl.ds(pl.multiple_of(zz * CORES * width, HEAD), CORES * width)]
        total_ref[...] += mm(heads, wo_all[zz].reshape(CORES * width, model))

    total_ref[...] = jnp.zeros_like(total_ref)
    tps(lambda tt: pl.when(put_off(tt))(lambda: start(mixed_copy(t, tt))))
    for s in range(first_left + 1, Z):
        both_sides(s, wo_relay)
    for s in range(1, first_left + 1):
        both_sides(s, wo_collect)
    mine.wait()

    def near(s, _):
        def side(d, _):
            zz = jnp.where(d == 0, z - s, z + s)

            @pl.when((zz >= 0) & (zz < Z) & ((s > 0) | (d == 0)))
            def _():
                @pl.when((s > first_left))
                def _():
                    wo_collect(zz)

                project(zz)

            return 0

        lax.fori_loop(0, 2, side, 0)
        return 0

    lax.fori_loop(0, Z, near, 0)
    mix_ref[...] = narrow(total_ref[...])

    zs(lambda zz: done_recv(line_copy(zz, zz)))
    result = line_in[0].astype(f32)
    for zz in range(1, Z):
        result = result + line_in[zz].astype(f32)
    exp_ref[...] = narrow(jnp.concatenate([result[:8], result[8:]], axis=1))

    zs(lambda zz: done_send(tok_copy(z, zz)))

    def drain(zz, _):
        for right in (lambda step: row_copy(zz, step), lambda step: wo_copy(zz, step, 0), lambda step: wo_copy(zz, step, 1)):
            pl.when((zz <= z) & (z + 1 < Z))(lambda: done_send(right(1)))
            pl.when((zz >= z) & (z >= 1))(lambda: done_send(right(-1)))
        done_send(row_sibling(zz, c))
        wo_siblings(zz, c, done_send)

        @pl.when(zz != z)
        def _():
            for i in range(2):
                eps(peers, lambda ee: done_send(wo_peer(zz, e, ee, i)))
            if relayed:
                for i in range(2):
                    done_send(wo_half(zz, e ^ (1 + i), i))

        return 0

    lax.fori_loop(0, Z, drain, 0)
    eps(others, lambda ee: done_send(tok_peer(e, ee)))
    eps(lambda ee: e >= 0, lambda ee: done_send(tok_sibling(ee, c)))
    eps(lambda ee: e < ee, lambda ee: done_send(state_copy(e, ee, 0)))
    eps(lambda ee: (e < ee) & (e > 0), lambda ee: done_send(state_copy(e, ee, 1)))
    eps(others, lambda ee: done_send(part_copy(e, ee)))
    done_send(part_sibling())
    zs(lambda zz: done_send(line_copy(z, zz)))
    tps(lambda tt: done_send(mixed_copy(t, tt)))


def body(
    mixer_input_rows,
    mixer_norm_gain,
    query_weight,
    key_weight,
    value_weight,
    write_strength_projection,
    decay_projection,
    head_decay_speed,
    largest_write_strength,
    extra_log_decay,
    head_norm_gain,
    mixer_output_weight,
    expert_input_rows,
    expert_norm_gain,
    routes,
    expert_route_weight,
    gate_weight,
    up_weight,
    down_weight,
):
    EP, T = lax.axis_size("ep"), lax.axis_size("tp")
    Z = T // CORES
    H = head_decay_speed.shape[0]
    width = H * HEAD
    block, model = mixer_input_rows.shape
    toks = expert_input_rows.shape[0]
    half = model // 2
    hidden = gate_weight.shape[2]
    assert block == BLOCK and toks == 8

    vmem = pl.BlockSpec(memory_space=pltpu.VMEM)
    anywhere = pl.BlockSpec(memory_space=pl.ANY)
    dma = pltpu.SemaphoreType.DMA
    V = pltpu.VMEM
    outs = [
        jax.ShapeDtypeStruct((block, model), bf16),
        jax.ShapeDtypeStruct((toks, model), bf16),
    ]
    small = [
        mixer_input_rows,
        mixer_norm_gain.reshape(1, model),
        write_strength_projection.T,
        decay_projection.T,
        largest_write_strength.reshape(1, H),
        head_decay_speed.reshape(1, H),
        extra_log_decay.T,
        head_norm_gain.reshape(1, HEAD),
        expert_input_rows,
        expert_norm_gain.reshape(1, model),
        routes.T,
        expert_route_weight.T,
    ]
    scratch = [
        *[V(v.shape, v.dtype) for v in small],
        dma((SMALL,)),
        V((2 * write_strength_projection.shape[1], model), bf16),
        V((model, width), bf16),
        V((model, width), bf16),
        V((model, width), bf16),
        V((model, hidden), bf16),
        V((model, hidden), bf16),
        V((hidden, model), bf16),
        V((Z, CORES, BLOCK, model), bf16),
        V((Z, CORES, width, model), bf16),
        V((EP, CORES, Z, 16, half + HEAD), bf16),
        V((CORES, EP, Z, 16, half), bf16),
        V((EP, Z, 16, half), bf16),
        V((EP, Z, 16, half), bf16),
        V((EP, Z, 16, half), bf16),
        V((Z, 16, half), bf16),
        V((Z, 16, half), bf16),
        V((Z, CORES * BLOCK, width), f32),
        V((Z, CORES * BLOCK, width), bf16),
        V((Z, H, HEAD, 2 * HEAD), f32),
        V((Z, H, HEAD, 2 * HEAD), bf16),
        V((H, HEAD, 2 * HEAD), f32),
        V((2, H, HEAD, HEAD), bf16),
        V((EP, 2, H, HEAD, HEAD), bf16),
        V((H, HEAD, HEAD), f32),
        V((BLOCK, model), f32),
        V((T, BLOCK, width), bf16),
        V((BLOCK, T * width), bf16),
        dma((8,)),
        *[dma((2, Z)), dma((Z,)), dma((Z,)), dma((Z,))],
        *[dma((2, Z, 2)), dma((Z, 2)), dma((Z, EP, 2)), dma((Z, EP, 2))],
        *[dma((Z, 2)), dma((Z, 2)), dma((Z, EP, 2)), dma((Z, EP, 2))],
        *[dma((Z,)), dma((Z,)), dma((EP,)), dma((EP,)), dma((EP,)), dma((EP,))],
        *[dma((EP, 2)), dma((EP, 2))],
        *[dma((1,)), dma((1,)), dma((EP,)), dma((EP,)), dma((Z,)), dma((Z,))],
        *[dma((T,)), dma((T,))],
    ]
    results = pl.pallas_call(
        functools.partial(loading_kernel, (EP, Z, H)),
        in_specs=[anywhere] * (SMALL + 7),
        out_specs=[vmem, vmem],
        out_shape=outs,
        scratch_shapes=scratch,
        compiler_params=pltpu.CompilerParams(
            collective_id=0, has_side_effects=True, vmem_limit_bytes=63 << 20
        ),
    )(
        *small,
        query_weight,
        key_weight,
        value_weight,
        mixer_output_weight,
        gate_weight,
        up_weight,
        down_weight,
    )
    return pl.pallas_call(
        hand_over,
        in_specs=[vmem, vmem],
        out_specs=[anywhere, anywhere],
        out_shape=outs,
        scratch_shapes=[dma((2,))],
    )(*results)


def hand_over(mix_in, exp_in, mix_out, exp_out, sem):
    copies = [
        pltpu.make_async_copy(mix_in, mix_out, sem.at[0]),
        pltpu.make_async_copy(exp_in, exp_out, sem.at[1]),
    ]
    for copy in copies:
        copy.start()
    for copy in copies:
        copy.wait()


def solution(mesh):
    placed = (
        P(("ep", "tp"), None),
        P(),
        P(None, "tp"),
        P(None, "tp"),
        P(None, "tp"),
        P(),
        P(),
        P("tp"),
        P("tp"),
        P("ep", "tp"),
        P(),
        P("tp", None),
        P(("ep", "tp"), None),
        P(),
        P(("ep", "tp"), None),
        P(("ep", "tp"), None),
        P("ep", None, "tp"),
        P("ep", None, "tp"),
        P("ep", "tp", None),
    )
    return jax.shard_map(
        body,
        mesh=mesh,
        in_specs=placed,
        out_specs=(P(("ep", "tp"), None), P(("ep", "tp"), None)),
        check_vma=False,
    )
```
